256 devices in a mesh: dp: 4 (over y), kv: 32 (over z, x), tp: 2 (over core).
Axes of the slice: x: 4, y: 4, z: 8, core: 2. Of those that a mesh axis runs over, the one named last changes fastest.
Arguments:
- tokens: bfloat16 [2048, 2048], P('dp', ('kv', 'tp')), parts along dimension 0, may hold values from -64 to 64, as said below
- lengths: int32 [256], P(('dp', 'kv', 'tp')), parts along dimension 0, may hold values from 1 to 8, 224 in all
- state: float32 [256, 16, 128, 128], P(('dp', 'kv', 'tp')), parts along dimension 0, may hold values from -1.8 to 1.8
- gain_first: float32 [2048], replicated, may hold values from 0.1 to 1.9
- first_gate: bfloat16 [2048, 5632], P(None, 'kv'), may hold values from -0.125 to 0.125
- first_up: bfloat16 [2048, 5632], P(None, 'kv'), may hold values from -0.125 to 0.125
- first_down: bfloat16 [5632, 2048], P('kv'), may hold values from -0.15625 to 0.15625
- gain_mix: float32 [2048], replicated, may hold values from 0.1 to 1.9
- query_weight: bfloat16 [2048, 2048], P(None, ('kv', 'tp')), may hold values from -0.125 to 0.125
- key_weight: bfloat16 [2048, 2048], P(None, ('kv', 'tp')), may hold values from -0.125 to 0.125
- value_weight: bfloat16 [2048, 2048], P(None, ('kv', 'tp')), may hold values from -0.125 to 0.125
- gating_weight: bfloat16 [2048, 2048], P(None, ('kv', 'tp')), may hold values from -0.125 to 0.125
- write_weight: bfloat16 [2048, 16], replicated, may hold values from -0.125 to 0.125
- forget_weight: bfloat16 [2048, 16], replicated, may hold values from -0.125 to 0.125
- forget_rate: float32 [16], replicated, may hold values from -4 to 1.5
- out_weight: bfloat16 [2048, 2048], P(None, ('kv', 'tp')), may hold values from -0.125 to 0.125
- gain_second: float32 [2048], replicated, may hold values from 0.1 to 1.9
- second_gate: bfloat16 [2048, 5632], P(None, 'kv'), may hold values from -0.125 to 0.125
- second_up: bfloat16 [2048, 5632], P(None, 'kv'), may hold values from -0.125 to 0.125
- second_down: bfloat16 [5632, 2048], P('kv'), may hold values from -0.15625 to 0.15625
Outputs:
- mixed_out: bfloat16 [2048, 2048], P('dp', ('kv', 'tp')), parts along dimension 0
- new_state: float32 [256, 16, 128, 128], P(('dp', 'kv', 'tp')), parts along dimension 0
The draws below stay inside these ranges and needn't reach their ends.
There are 4 independent parts, one for each index of `dp`. The reference program is written for one: setup_inputs(seed, part) draws one part's arguments, and reference() takes and returns one part's arrays. A program takes and returns all parts, laid end to end along the dimension named above; an argument that names none is the same for every part. Nothing has to cross between parts.
Inputs may be any that keep to these rules, and one draw needn't show every extreme that they name: Activations of the new tokens. `lengths`: the live new tokens of each sequence; within each independent group of 64 sequences (one part along dp) they sum to seven halves of 64, rounded down, and some sequence of each group has all 8 live.
All inputs are finite; a program needn't handle non-finite values.
Results may differ from the reference program's by a relative error of at most 0.0058.
Values may be sent and summed in bfloat16 or wider, within the bound.
A program may use at most 64 MiB of HBM per device.

```python
import math
import jax
import jax.numpy as jnp
import numpy as np
from jax import lax

D = 2048
HEADS = 16
HEAD = 128
FF = 5632
BLK = 8
SEQS = 64
ROWS = 512


def draw_tokens(key, part):
    key_base = jax.random.fold_in(key, 17)
    key_one, key_two, key_three = jax.random.split(key_base, 3)
    columns = jnp.arange(D, dtype=jnp.float32)
    rough_cols = jnp.exp(jax.random.uniform(key_two, (1, D), jnp.float32, -0.35, 0.35))
    col_scale = jnp.exp(math.log(5.0) * (columns[None, :] / D - 0.5)) * rough_cols
    base = jnp.clip(jax.random.normal(key_one, (ROWS, D), jnp.float32), -5.0, 5.0)
    row_scale = jnp.exp(jax.random.uniform(key_three, (ROWS, 1), jnp.float32, math.log(0.4), math.log(4.0)))
    return (base * row_scale * col_scale).astype(jnp.bfloat16)


def spiked(array, key, source, target, blocks, factor):
    owner, partner = [(jnp.arange(array.shape[position]) // (array.shape[position] // blocks)).reshape([-1 if axis == position else 1 for axis in range(array.ndim)]) for position in (source, target)]
    chosen = jax.random.permutation(key, blocks)[partner]
    strong = (owner == chosen) | (owner == (partner + blocks // 2) % blocks)
    return jnp.where(strong, factor * array, array)


def steps_of(own_key, dims, pieces, smallest, high):
    level = 1.0
    for axis_at, parts in pieces:
        heights = jax.random.uniform(jax.random.fold_in(jax.random.fold_in(own_key, 6), axis_at), (parts,), jnp.float32, smallest / len(pieces), high / len(pieces))
        level = level * jnp.repeat(jnp.exp(heights), dims[axis_at] // parts).reshape((-1,) + (1,) * (len(dims) - 1 - axis_at))
    return level


def profile(count, total, most, skew):
    loads = [(1 << 20) // math.isqrt(standing ** skew) + 1 for standing in range(2, count + 1)]
    spare, given = total - most - (count - 1), [1] * (count - 1)
    while spare > 0:
        free = [i for i in range(count - 1) if given[i] < most]
        whole, left = sum([loads[i] for i in free]), spare
        for i in free:
            addition = min(most - given[i], max(1, left * loads[i] // whole), spare)
            given[i] = given[i] + addition
            spare = spare - addition
    return np.array([most] + given)


def uneven_parts(stream_key, number_of, total, most, slope):
    if number_of == 2:
        one = jax.random.randint(stream_key, (), max(1, total - most), min(most, total - 1) + 1)
        return jnp.stack([one, total - one])
    tallies = jnp.asarray(profile(number_of, total, most, slope), jnp.int32)
    pairs = (number_of - 1) // 2
    source_of, taker = tallies[1:1 + 2 * pairs:2], tallies[2:2 + 2 * pairs:2]
    slack = jnp.minimum(source_of - 1, most - taker)
    passed = jax.random.randint(jax.random.fold_in(stream_key, 1), (pairs,), 0, 1 << 20) % (slack + 1)
    tallies = tallies.at[1:1 + 2 * pairs:2].set(source_of - passed).at[2:2 + 2 * pairs:2].set(taker + passed)
    return tallies[jax.random.permutation(jax.random.fold_in(stream_key, 2), number_of)]


def gaussian(own_key, extent, spread, most, shards=(), kind=jnp.bfloat16):
    loudness = steps_of(own_key, extent, shards, -0.22, 0.18) if shards else 1.0
    values = jax.random.normal(own_key, extent, jnp.float32) * spread * loudness
    return jnp.minimum(jnp.maximum(values, -most), most).astype(kind)


def gaussian_with(stream_key, shape, scale, most, cuts, heavy, held_as=jnp.bfloat16):
    values = scale * jax.random.normal(stream_key, shape, jnp.float32)
    if cuts:
        values = values * steps_of(stream_key, shape, cuts, -0.22, 0.18)
    return jnp.clip(spiked(values, jax.random.fold_in(stream_key, 3), *heavy), -most, most).astype(held_as)


def setup_inputs(seed: int = 0, part: int = 0) -> dict:
    keys = jax.random.split(jax.random.key(seed), 21)
    part_splits = jax.random.split(jax.random.fold_in(keys[20], part), 21)
    tokens = draw_tokens(jax.random.fold_in(jax.random.fold_in(keys[20], part), 71), part)
    lengths = uneven_parts(part_splits[1], SEQS, SEQS * 7 // 2, BLK, 2).astype(jnp.int32)
    state = gaussian(part_splits[2], (SEQS, HEADS, HEAD, HEAD), 0.3, 1.8, ((0, 64),), jnp.float32)
    gain_first = jnp.clip(1.0 + 0.18 * jax.random.normal(keys[3], (D,), jnp.float32), 0.1, 1.9)
    first_gate = gaussian(keys[4], (D, FF), D ** -0.5, 0.125, ((1, 32),))
    first_up = gaussian(keys[5], (D, FF), D ** -0.5, 0.125, ((1, 32),))
    first_down = gaussian_with(keys[6], (FF, D), FF ** -0.5, 0.15625, ((0, 32),), (0, 1, 32, 2.75))
    gain_mix = jnp.clip(1.0 + 0.18 * jax.random.normal(keys[7], (D,), jnp.float32), 0.1, 1.9)
    query_weight = gaussian(keys[8], (D, HEADS * HEAD), D ** -0.5, 0.125, ((1, 64),))
    key_weight = gaussian(keys[9], (D, HEADS * HEAD), D ** -0.5, 0.125, ((1, 64),))
    value_weight = gaussian(keys[10], (D, HEADS * HEAD), D ** -0.5, 0.125, ((1, 64),))
    gating_weight = gaussian(keys[11], (D, HEADS * HEAD), D ** -0.5, 0.125, ((1, 64),))
    write_weight = gaussian(keys[12], (D, HEADS), D ** -0.5, 0.125)
    forget_weight = gaussian(keys[13], (D, HEADS), D ** -0.5, 0.125)
    forget_rate = jnp.clip(jax.random.uniform(keys[14], (HEADS,), jnp.float32, -4.0, 1.5), -4.0, 1.5)
    out_weight = gaussian(keys[15], (HEADS * HEAD, D), (HEADS * HEAD) ** -0.5, 0.125, ((1, 64),))
    gain_second = jnp.clip(1.0 + 0.18 * jax.random.normal(keys[16], (D,), jnp.float32), 0.1, 1.9)
    second_gate = gaussian(keys[17], (D, FF), D ** -0.5, 0.125, ((1, 32),))
    second_up = gaussian(keys[18], (D, FF), D ** -0.5, 0.125, ((1, 32),))
    second_down = gaussian_with(keys[19], (FF, D), FF ** -0.5, 0.15625, ((0, 32),), (0, 1, 32, 2.75))
    return {"tokens": tokens, "lengths": lengths, "state": state, "gain_first": gain_first, "first_gate": first_gate, "first_up": first_up, "first_down": first_down, "gain_mix": gain_mix, "query_weight": query_weight, "key_weight": key_weight, "value_weight": value_weight, "gating_weight": gating_weight, "write_weight": write_weight, "forget_weight": forget_weight, "forget_rate": forget_rate, "out_weight": out_weight, "gain_second": gain_second, "second_gate": second_gate, "second_up": second_up, "second_down": second_down}


EPSILON = 1e-06

def feed_forward(hidden_in, gain, w_gate, w_up, w_down):
    values = hidden_in.astype(jnp.float32)
    row_scale = lax.rsqrt(lax.optimization_barrier(jnp.mean(values * values, axis=1, keepdims=True)) + EPSILON)
    scaled = (values * gain).astype(jnp.bfloat16)
    gate_act = jnp.dot(scaled, w_gate, preferred_element_type=jnp.float32) * row_scale
    up_act = jnp.dot(scaled, w_up, preferred_element_type=jnp.float32) * row_scale
    hidden = (jax.nn.silu(gate_act) * up_act).astype(jnp.bfloat16)
    result = jnp.dot(hidden, w_down, preferred_element_type=jnp.float32)
    return (values + 0.5 * result).astype(jnp.bfloat16)

def delta_block(query, key_in, value, gating, write_pre, forget_pre, rates, live, state):
    seq_count, block_len, head_count, head_size = query.shape
    precise = lax.Precision.HIGHEST
    query_unit = query * lax.rsqrt(lax.optimization_barrier(jnp.sum(query * query, axis=-1, keepdims=True)) + EPSILON) / math.sqrt(head_size)
    key_unit = key_in * lax.rsqrt(lax.optimization_barrier(jnp.sum(key_in * key_in, axis=-1, keepdims=True)) + EPSILON)
    live_rows = live[:, :, None]
    write_gate = jax.nn.sigmoid(write_pre) * live_rows
    forget = -jnp.exp(rates)[None, None, :] * jax.nn.softplus(forget_pre) * live_rows
    cumulative = jnp.cumsum(forget, axis=1)
    cum_heads = jnp.transpose(cumulative, (0, 2, 1))
    positions = jnp.arange(block_len)
    causal = positions[:, None] >= positions[None, :]
    strict = positions[:, None] > positions[None, :]
    differ = jnp.minimum(cum_heads[:, :, :, None] - cum_heads[:, :, None, :], 0.0)
    decay_mat = jnp.where(causal, jnp.exp(differ), 0.0)
    key_dots = jnp.einsum('sthd,suhd->shtu', key_unit, key_unit, precision=precise)
    write_heads = jnp.transpose(write_gate, (0, 2, 1))
    strict_part = jnp.where(strict, write_heads[:, :, :, None] * decay_mat * key_dots, 0.0)
    identity = jnp.eye(block_len, dtype=jnp.float32)
    squared = jnp.einsum('shtu,shuv->shtv', strict_part, strict_part, precision=precise)
    fourth = jnp.einsum('shtu,shuv->shtv', squared, squared, precision=precise)
    inverse = jnp.einsum('shtu,shuv->shtv', identity - strict_part, identity + squared, precision=precise)
    inverse = jnp.einsum('shtu,shuv->shtv', inverse, identity + fourth, precision=precise)
    growth = jnp.exp(cumulative)
    target = jnp.einsum('shtu,suhv->sthv', inverse, write_gate[..., None] * value, precision=precise)
    key_mix = jnp.einsum('shtu,suhk->sthk', inverse, (write_gate * growth)[..., None] * key_unit, precision=precise)
    update = target - jnp.einsum('sthk,shkv->sthv', key_mix, state, precision=precise)
    scores = jnp.einsum('sthd,suhd->shtu', query_unit, key_unit, precision=precise) * decay_mat
    attend = jnp.einsum('sthk,shkv->sthv', query_unit * growth[..., None], state, precision=precise)
    attend = attend + jnp.einsum('shtu,suhv->sthv', scores, update, precision=precise)
    final_cum = cumulative[:, -1:, :]
    fading = jnp.exp(final_cum - cumulative)
    new_state = jnp.exp(final_cum[:, 0, :])[:, :, None, None] * state
    new_state = new_state + jnp.einsum('sthk,sthv->shkv', key_unit * fading[..., None], update, precision=precise)
    normed = attend * lax.rsqrt(lax.optimization_barrier(jnp.mean(attend * attend, axis=-1, keepdims=True)) + EPSILON)
    normed = normed * jax.nn.silu(gating) * live[:, :, None, None]
    mixed_heads = normed.reshape(seq_count * block_len, head_count * head_size).astype(jnp.bfloat16)
    return (mixed_heads, new_state)

def reference(tokens, lengths, state, gain_first, first_gate, first_up, first_down, gain_mix, query_weight, key_weight, value_weight, gating_weight, write_weight, forget_weight, forget_rate, out_weight, gain_second, second_gate, second_up, second_down):
    after_first = feed_forward(tokens, gain_first, first_gate, first_up, first_down)
    values = after_first.astype(jnp.float32)
    mix_scale = lax.rsqrt(lax.optimization_barrier(jnp.mean(values * values, axis=1, keepdims=True)) + EPSILON)
    mix_in = (values * gain_mix).astype(jnp.bfloat16)

    def project(matrix):
        return jnp.dot(mix_in, matrix, preferred_element_type=jnp.float32) * mix_scale
    query = project(query_weight).reshape(SEQS, BLK, HEADS, HEAD)
    key_in = project(key_weight).reshape(SEQS, BLK, HEADS, HEAD)
    value = project(value_weight).reshape(SEQS, BLK, HEADS, HEAD)
    gating = project(gating_weight).reshape(SEQS, BLK, HEADS, HEAD)
    write_pre = project(write_weight).reshape(SEQS, BLK, HEADS)
    forget_pre = project(forget_weight).reshape(SEQS, BLK, HEADS)
    positions = jnp.arange(BLK, dtype=jnp.int32)
    live = (positions[None, :] < lengths[:, None]).astype(jnp.float32)
    mixed_heads, new_state = delta_block(query, key_in, value, gating, write_pre, forget_pre, forget_rate, live, state)
    half_cols = HEADS * HEAD // 2
    running = values
    for half_index in range(2):
        portion = jnp.dot(mixed_heads[:, half_index * half_cols:(half_index + 1) * half_cols], out_weight[half_index * half_cols:(half_index + 1) * half_cols], preferred_element_type=jnp.float32)
        rounded = lax.optimization_barrier(portion.astype(jnp.bfloat16)).astype(jnp.float32)
        running = running + rounded
    after_mix = running.astype(jnp.bfloat16)
    mixed_out = feed_forward(after_mix, gain_second, second_gate, second_up, second_down)
    return (mixed_out, new_state)
```

```python
import math

import jax
import jax.numpy as jnp
from jax import lax
from jax.experimental import pallas as pl
from jax.experimental.pallas import tpu as pltpu
from jax.sharding import PartitionSpec as P

HEADS = 16
HEAD = 128
BLK = 8
D = 2048
NX = 4
NZ = 8
CHIPS = NX * NZ
ROWS = CHIPS * BLK
EPSILON = 1e-06
F32 = jnp.float32
BF16 = jnp.bfloat16
HIGH = lax.Precision.HIGHEST
DZ_FAR = (4, 3, -3, 2, -2, 1, -1, 0)


def lanes_swapped(tiles):
    rows = tiles[0].shape[0]
    lane = lax.broadcasted_iota(jnp.int32, (rows, 128), 1)
    out = list(tiles)
    for step in (2, 1):
        width = step * 32
        low = (lane & width) == 0
        for i in range(4):
            if i & step:
                continue
            a, b = out[i], out[i + step]
            out[i] = jnp.where(low, a, pltpu.roll(b, width, 1))
            out[i + step] = jnp.where(low, pltpu.roll(a, 128 - width, 1), b)
    return out


def wrapped(dz):
    return (dz + 3) % NZ - 3


def place(dx, dz):
    return (dx % NX) * NZ + dz % NZ


def children(half, dx, dz):
    sign = 1 if half == 0 else -1
    dx, dz = dx % NX, wrapped(dz)
    found = []
    if dx == 0:
        if dz == 0:
            found += [(0, sign * 2), (0, -sign * 3), (0, sign * 3), (0, -sign * 2), (0, 1), (0, -1)]
        if dz == sign * 2:
            found.append((0, 4))
        found += [(1, dz), (-1, dz)]
    elif dx == sign % NX:
        found.append((2, dz))
    return found


ARRIVALS = (
    [(0, 1), (0, -1), (1, 0), (-1, 0), (0, 2), (0, -2)]
    + [(1, 1), (-1, 1), (1, -1), (-1, -1), (0, 3), (0, -3)]
    + [(1, 2), (-1, 2), (1, -2), (-1, -2), (0, 4)]
    + [(1, 3), (-1, 3), (1, -3), (-1, -3), (2, 0), (2, 1), (2, -1)]
    + [(1, 4), (-1, 4), (2, 2), (2, -2), (2, 3), (2, -3), (2, 4)]
)


class Torus:
    def __init__(self):
        self.kv = lax.axis_index("kv")
        self.tp = lax.axis_index("tp")
        self.x = lax.rem(self.kv, NX)
        self.z = lax.div(self.kv, NX)

    def at(self, dx, dz):
        return lax.rem(self.z + dz % NZ, NZ) * NX + lax.rem(self.x + dx % NX, NX)


def send(src, dst, send_sem, recv_sem, target):
    pltpu.make_async_remote_copy(
        src_ref=src,
        dst_ref=dst,
        send_sem=send_sem,
        recv_sem=recv_sem,
        device_id=target,
        device_id_type=pl.DeviceIdType.MESH,
    ).start()


def arrived(ref, sem):
    pltpu.make_async_copy(ref, ref, sem).wait()


def gather(torus, buf, send_sem, recv_sem):
    def pass_on(half, dx, dz):
        source = torus.at(-dx, -dz)
        for cx, cz in children(half, dx, dz):
            send(
                buf.at[source, half],
                buf.at[source, half],
                send_sem,
                recv_sem.at[half, place(cx, cz)],
                {"kv": torus.at(cx - dx, cz - dz)},
            )

    for half in range(2):
        pass_on(half, 0, 0)
    for dx, dz in ARRIVALS:
        for half in range(2):
            arrived(buf.at[torus.at(-dx, -dz), half], recv_sem.at[half, place(dx, dz)])
            pass_on(half, dx, dz)


def sum_at_owner(torus, part, relay, column, cross, final, stage_x, stage_z, send_sem, recv_sem):
    def slot(dz):
        return dz % NZ

    for dz in DZ_FAR:
        for half in range(2):
            sign = 1 if half == 0 else -1
            send(
                part.at[torus.at(2, -dz), half],
                relay.at[half, slot(dz)],
                send_sem,
                recv_sem.at[half, slot(dz)],
                {"kv": torus.at(-sign, 0)},
            )
        for half in range(2):
            sign = 1 if half == 0 else -1
            send(
                part.at[torus.at(sign, -dz), half],
                column.at[half, 0, slot(dz)],
                send_sem,
                recv_sem.at[half, 8 + slot(dz)],
                {"kv": torus.at(sign, 0)},
            )
    for dz in DZ_FAR:
        for half in range(2):
            sign = 1 if half == 0 else -1
            arrived(relay.at[half, slot(dz)], recv_sem.at[half, slot(dz)])
            total = part[torus.at(-sign, -dz), half].astype(F32) + relay[half, slot(dz)].astype(F32)
            stage_x[half, slot(dz)] = total.astype(BF16)
            send(
                stage_x.at[half, slot(dz)],
                column.at[half, 1, slot(dz)],
                send_sem,
                recv_sem.at[half, 16 + slot(dz)],
                {"kv": torus.at(-sign, 0)},
            )
    sums = [None, None]
    for dz in DZ_FAR:
        for half in range(2):
            sign = 1 if half == 0 else -1
            arrived(column.at[half, 0, slot(dz)], recv_sem.at[half, 8 + slot(dz)])
            arrived(column.at[half, 1, slot(dz)], recv_sem.at[half, 16 + slot(dz)])
            total = (
                part[torus.at(0, -dz), half].astype(F32)
                + column[half, 0, slot(dz)].astype(F32)
                + column[half, 1, slot(dz)].astype(F32)
            )
            if dz == 0:
                sums[half] = total
                continue
            if dz == 2 * sign:
                arrived(cross.at[half], recv_sem.at[half, 28])
                total = total + cross[half].astype(F32)
            stage_z[half, slot(dz)] = total.astype(BF16)
            if dz == 4:
                send(
                    stage_z.at[half, slot(dz)],
                    cross.at[half],
                    send_sem,
                    recv_sem.at[half, 28],
                    {"kv": torus.at(0, -2 * sign)},
                )
            else:
                send(
                    stage_z.at[half, slot(dz)],
                    final.at[half, slot(dz)],
                    send_sem,
                    recv_sem.at[half, 24 + slot(dz)],
                    {"kv": torus.at(0, -dz)},
                )
    for dz in (3, -3, 2, -2, 1, -1):
        for half in range(2):
            arrived(final.at[half, slot(dz)], recv_sem.at[half, 24 + slot(dz)])
            sums[half] = sums[half] + final[half, slot(dz)].astype(F32)
    return sums


def unpack(buf, gain_ref, scaled_ref, squares_ref):
    squares_ref[...] = jnp.zeros_like(squares_ref)

    def body(k, carry):
        cols = pl.ds(pl.multiple_of(k * 128, 128), 128)
        tiles = [buf[2 * k + j // 2, j % 2].astype(F32) for j in range(4)]
        for q, tile in enumerate(lanes_swapped(tiles)):
            rows = pl.ds(64 * q, 64)
            scaled_ref[rows, cols] = (tile * gain_ref[:, cols]).astype(BF16)
            squares_ref[rows, :] += tile * tile
        return carry

    lax.fori_loop(0, D // 128, body, 0)
    total = jnp.sum(squares_ref[...], axis=1, keepdims=True)
    return lax.rsqrt(total / D + EPSILON)


def half_step(torus, buf, gain_ref, gate_ref, up_ref, down_ref, weight_waits, scaled_ref, squares_ref,
              part, sum_refs, send_sem, recv_sem):
    row_scale = unpack(buf, gain_ref, scaled_ref, squares_ref)
    for wait in weight_waits:
        wait()
    scaled = scaled_ref[...]
    gate_act = jnp.dot(scaled, gate_ref[...], preferred_element_type=F32) * row_scale
    up_act = jnp.dot(scaled, up_ref[...], preferred_element_type=F32) * row_scale
    hidden = (jax.nn.silu(gate_act) * up_act).astype(BF16)

    def body(k, carry):
        cols = pl.ds(pl.multiple_of(k * 256, 256), 256)
        product = jnp.dot(hidden, down_ref[:, cols], preferred_element_type=F32)
        for side in range(2):
            tiles = [product[64 * q : 64 * q + 64, 128 * side : 128 * side + 128] for q in range(4)]
            for j, tile in enumerate(lanes_swapped(tiles)):
                part[4 * k + 2 * side + j // 2, j % 2] = tile.astype(BF16)
        return carry

    lax.fori_loop(0, D // 256, body, 0)
    return sum_at_owner(torus, part, *sum_refs, send_sem, recv_sem)


def spread(rows, first):
    parts = [jnp.broadcast_to(rows[:, first + h : first + h + 1], (BLK, 128)) for h in range(HEADS)]
    return jnp.concatenate(parts, axis=0)


def delta(owned, gates_in, rates, live, state, fresh):
    query, key, value, gating = owned
    write_rows = jax.nn.sigmoid(gates_in) * live
    forget_rows = -jnp.exp(rates) * jax.nn.softplus(gates_in) * live
    write = spread(write_rows, 0)
    forget = spread(forget_rows, HEADS)
    query_unit = query * lax.rsqrt(jnp.sum(query * query, axis=1, keepdims=True) + EPSILON)
    query_unit = query_unit / math.sqrt(HEAD)
    key_unit = key * lax.rsqrt(jnp.sum(key * key, axis=1, keepdims=True) + EPSILON)
    row = lax.broadcasted_iota(jnp.int32, (128, 128), 0)
    col = lax.broadcasted_iota(jnp.int32, (128, 128), 1)
    same = (row >> 3) == (col >> 3)
    causal = same & (col <= row)
    strict = same & (col < row)
    identity = jnp.where(row == col, 1.0, 0.0)

    def dot(a, b):
        return jnp.dot(a, b, precision=HIGH, preferred_element_type=F32)

    def dot_nt(a, b):
        return lax.dot_general(
            a, b, (((1,), (1,)), ((), ())), precision=HIGH, preferred_element_type=F32
        )

    cumulative = dot(jnp.where(causal, 1.0, 0.0), forget)
    decay = jnp.where(causal, jnp.exp(jnp.minimum(cumulative - cumulative.T, 0.0)), 0.0)
    strict_part = jnp.where(strict, write * decay * dot_nt(key_unit, key_unit), 0.0)
    squared = dot(strict_part, strict_part)
    fourth = dot(squared, squared)
    inverse = dot(dot(identity - strict_part, identity + squared), identity + fourth)
    growth = jnp.exp(cumulative)
    target = dot(inverse, write * value)
    key_mix = dot(inverse, write * growth * key_unit)
    scores = dot_nt(query_unit, key_unit) * decay
    grown = query_unit * growth
    by_head = cumulative.reshape(HEADS, BLK, 128)
    last = by_head[:, BLK - 1 : BLK, :]
    fading = jnp.exp(last - by_head).reshape(128, 128)
    faded = key_unit * fading
    kept = jnp.exp(last)
    updates, reads = [], []
    for h in range(HEADS):
        rows = slice(8 * h, 8 * h + 8)
        both = jnp.concatenate([key_mix[rows], grown[rows]], axis=0)
        seen = dot(both, state[h])
        update = target[rows] - seen[:BLK]
        updates.append(update)
        reads.append(seen[BLK:])
        gained = lax.dot_general(
            faded[rows], update, (((0,), (0,)), ((), ())), precision=HIGH, preferred_element_type=F32
        )
        fresh[h] = kept[h] * state[h] + gained
    attend = jnp.concatenate(reads, axis=0) + dot(scores, jnp.concatenate(updates, axis=0))
    normed = attend * lax.rsqrt(jnp.mean(attend * attend, axis=1, keepdims=True) + EPSILON)
    return normed * jax.nn.silu(gating) * jnp.concatenate([live] * HEADS, axis=0)


def layer(
    tok, live, rates, gain_first, gain_mix, gain_second,
    gate1, up1, down1, gate2, up2, down2, proj, outw, wf, state,
    out, new_state,
    buf_a, buf_c, buf_m, buf_g, scaled, squares, part1, part2,
    relay1, column1, cross1, final1, relay2, column2, cross2, final2,
    stage_x1, stage_z1, stage_x2, stage_z2,
    v_gate1, v_up1, v_down1, v_gate2, v_up2, v_down2, v_proj, v_out, v_wf, v_state, v_fresh,
    outgoing, incoming, gates, last_stage,
    local_sem, send_sem, recv_ag, recv_rs, recv_x, pair_sem,
):
    torus = Torus()
    kv, tp = torus.kv, torus.tp
    other = 1 - tp

    loads = {}
    for n, (name, src, dst) in enumerate(
        [
            ("gate1", gate1, v_gate1), ("up1", up1, v_up1), ("down1", down1, v_down1),
            ("proj", proj, v_proj.at[tp]), ("out", outw, v_out.at[tp]), ("wf", wf, v_wf),
            ("state", state, v_state),
            ("gate2", gate2, v_gate2), ("up2", up2, v_up2), ("down2", down2, v_down2),
        ]
    ):
        loads[name] = pltpu.make_async_copy(src, dst, local_sem.at[n])
        loads[name].start()

    barrier = pltpu.get_barrier_semaphore()
    for d in range(1, CHIPS):
        pl.semaphore_signal(
            barrier, inc=1, device_id={"kv": lax.rem(kv + d, CHIPS)}, device_id_type=pl.DeviceIdType.MESH
        )
    pl.semaphore_signal(barrier, inc=1, device_id={"tp": other}, device_id_type=pl.DeviceIdType.MESH)
    pl.semaphore_wait(barrier, CHIPS)

    send(tok.at[other], buf_a.at[kv, tp], pair_sem.at[0], pair_sem.at[1], {"tp": other})
    buf_a[kv, tp] = tok[tp]
    arrived(buf_a.at[kv, other], pair_sem.at[1])
    gather(torus, buf_a, send_sem.at[0], recv_ag.at[0])
    loads["proj"].wait()
    loads["out"].wait()
    send(v_proj.at[tp], v_proj.at[tp], pair_sem.at[2], pair_sem.at[3], {"tp": other})
    send(v_out.at[tp], v_out.at[tp], pair_sem.at[4], pair_sem.at[5], {"tp": other})

    sums = half_step(
        torus, buf_a, gain_first, v_gate1, v_up1, v_down1,
        [loads["gate1"].wait, loads["up1"].wait, loads["down1"].wait],
        scaled, squares, part1, (relay1, column1, cross1, final1, stage_x1, stage_z1),
        send_sem.at[1], recv_rs.at[0],
    )
    for half in range(2):
        buf_c[kv, half] = (buf_a[kv, half].astype(F32) + 0.5 * sums[half]).astype(BF16)

    gather(torus, buf_c, send_sem.at[2], recv_ag.at[1])
    mix_scale = unpack(buf_c, gain_mix, scaled, squares)
    arrived(v_proj.at[other], pair_sem.at[3])
    loads["wf"].wait()
    mix_in = scaled[...]
    for t in range(2):
        product = jnp.dot(mix_in, v_proj[t], preferred_element_type=F32) * mix_scale
        outgoing[:, t] = product.reshape(CHIPS, BLK, 128).astype(BF16)
    gates[...] = jnp.dot(mix_in, v_wf[...], preferred_element_type=F32) * mix_scale
    for d in range(1, CHIPS):
        peer = lax.rem(kv + d, CHIPS)
        send(outgoing.at[peer], incoming.at[kv], send_sem.at[3], recv_x.at[d], {"kv": peer})
    incoming[kv] = outgoing[kv]
    gates_in = gates[pl.ds(pl.multiple_of(kv * BLK, BLK), BLK), :]
    loads["state"].wait()
    for d in range(1, CHIPS):
        arrived(incoming.at[lax.rem(kv + CHIPS - d, CHIPS)], recv_x.at[d])
    tiles = incoming[...].astype(F32).reshape(HEADS, 4, BLK, 128)
    owned = lanes_swapped([tiles[:, j].reshape(128, 128) for j in range(4)])
    mixed = delta(owned, gates_in, rates[...], live[...], v_state, v_fresh)
    for h in range(HEADS):
        lanes = slice(128 * (h % 8), 128 * (h % 8) + 128)
        buf_m[kv, h // 8, :, lanes] = mixed[8 * h : 8 * h + 8].astype(BF16)
    save = pltpu.make_async_copy(v_fresh, new_state, local_sem.at[10])
    save.start()

    gather(torus, buf_m, send_sem.at[4], recv_ag.at[2])
    arrived(v_out.at[other], pair_sem.at[5])
    mixes = [jnp.zeros((64, 128), F32), jnp.zeros((64, 128), F32)]
    weight = v_out[0] + v_out[1]
    for half in range(2):
        heads_half = buf_m[:, half].astype(F32).reshape(ROWS, D // 2).astype(BF16)
        product = jnp.dot(
            heads_half, weight[half * (D // 2) : (half + 1) * (D // 2)], preferred_element_type=F32
        )
        tiles = lanes_swapped([product[64 * q : 64 * q + 64] for q in range(4)])
        for t in range(2):
            mixes[t] = mixes[t] + tiles[t].astype(BF16).astype(F32)
    for half in range(2):
        buf_g[kv, half] = (buf_c[kv, half].astype(F32) + mixes[half]).astype(BF16)

    gather(torus, buf_g, send_sem.at[5], recv_ag.at[3])
    sums = half_step(
        torus, buf_g, gain_second, v_gate2, v_up2, v_down2,
        [loads["gate2"].wait, loads["up2"].wait, loads["down2"].wait],
        scaled, squares, part2, (relay2, column2, cross2, final2, stage_x2, stage_z2),
        send_sem.at[6], recv_rs.at[1],
    )
    for half in range(2):
        last_stage[half] = (buf_g[kv, half].astype(F32) + 0.5 * sums[half]).astype(BF16)
    send(last_stage.at[other], out.at[tp], pair_sem.at[6], pair_sem.at[7], {"tp": other})
    out[tp] = last_stage[tp]
    arrived(out.at[other], pair_sem.at[7])

    arrived(tok.at[other], pair_sem.at[0])
    arrived(v_proj.at[tp], pair_sem.at[2])
    arrived(v_out.at[tp], pair_sem.at[4])
    arrived(last_stage.at[other], pair_sem.at[6])
    everything = pl.ds(0, CHIPS - 1)
    for n, ref in ((0, buf_a), (1, part1), (2, buf_c), (3, incoming), (4, buf_m), (5, buf_g), (6, part2)):
        arrived(ref.at[everything], send_sem.at[n])
    save.wait()


def run_layer(*arrays):
    bf, fl = BF16, F32
    dma = pltpu.SemaphoreType.DMA
    whole = (CHIPS, 2, 64, 128)
    in_vmem = pl.BlockSpec(memory_space=pltpu.VMEM)
    in_hbm = pl.BlockSpec(memory_space=pl.ANY)
    ff = 176
    sum_set = [
        pltpu.VMEM((2, 8, 64, 128), bf), pltpu.VMEM((2, 2, 8, 64, 128), bf),
        pltpu.VMEM((2, 64, 128), bf), pltpu.VMEM((2, 8, 64, 128), bf),
    ]
    return pl.pallas_call(
        layer,
        out_shape=(
            jax.ShapeDtypeStruct((2, 64, 128), bf),
            jax.ShapeDtypeStruct((HEADS, HEAD, HEAD), fl),
        ),
        in_specs=[in_vmem] * 6 + [in_hbm] * 10,
        out_specs=(in_vmem, in_hbm),
        scratch_shapes=[
            pltpu.VMEM(whole, bf), pltpu.VMEM(whole, bf),
            pltpu.VMEM((CHIPS, 2, BLK, D // 2), bf), pltpu.VMEM(whole, bf),
            pltpu.VMEM((ROWS, D), bf), pltpu.VMEM((ROWS, 128), fl),
            pltpu.VMEM(whole, bf), pltpu.VMEM(whole, bf),
            *sum_set, *sum_set,
            *([pltpu.VMEM((2, 8, 64, 128), bf)] * 4),
            pltpu.VMEM((D, ff), bf), pltpu.VMEM((D, ff), bf), pltpu.VMEM((ff, D), bf),
            pltpu.VMEM((D, ff), bf), pltpu.VMEM((D, ff), bf), pltpu.VMEM((ff, D), bf),
            pltpu.VMEM((2, D, 128), bf), pltpu.VMEM((2, D, 128), bf), pltpu.VMEM((D, 128), bf),
            pltpu.VMEM((HEADS, HEAD, HEAD), fl), pltpu.VMEM((HEADS, HEAD, HEAD), fl),
            pltpu.VMEM((CHIPS, 2, BLK, 128), bf), pltpu.VMEM((CHIPS, 2, BLK, 128), bf),
            pltpu.VMEM((ROWS, 128), fl), pltpu.VMEM((2, 64, 128), bf),
            dma((11,)), dma((7,)), dma((4, 2, 32)), dma((2, 2, 32)), dma((32,)), dma((8,)),
        ],
        compiler_params=pltpu.CompilerParams(
            collective_id=0, has_side_effects=True, vmem_limit_bytes=56 * 1024 * 1024
        ),
        name="layer",
    )(*arrays)


def per_device(
    tokens,
    lengths,
    state,
    gain_first,
    first_gate,
    first_up,
    first_down,
    gain_mix,
    query_weight,
    key_weight,
    value_weight,
    gating_weight,
    write_weight,
    forget_weight,
    forget_rate,
    out_weight,
    gain_second,
    second_gate,
    second_up,
    second_down,
):
    tok = tokens.reshape(4, 8, 2, BLK, 32).transpose(2, 1, 3, 0, 4).reshape(2, 64, 128)
    live = (jnp.arange(BLK, dtype=jnp.int32) < lengths[0]).astype(F32)
    live = jnp.broadcast_to(live[:, None], (BLK, 128))
    rates = jnp.pad(forget_rate[None, :], ((0, 0), (HEADS, 128 - 2 * HEADS)))
    proj = jnp.concatenate([query_weight, key_weight, value_weight, gating_weight], axis=1)
    blank = jnp.zeros_like(out_weight)
    first = lax.axis_index("tp") == 0
    outw = jnp.concatenate(
        [jnp.where(first, out_weight, blank), jnp.where(first, blank, out_weight), blank, blank], axis=1
    )
    wf = jnp.pad(
        jnp.concatenate([write_weight, forget_weight], axis=1), ((0, 0), (0, 128 - 2 * HEADS))
    )
    out, new_state = run_layer(
        tok, live, rates, gain_first[None, :], gain_mix[None, :], gain_second[None, :],
        first_gate, first_up, first_down, second_gate, second_up, second_down,
        proj, outw, wf, state.reshape(HEADS, HEAD, HEAD),
    )
    mixed_out = out.reshape(2, 8, BLK, 4, 32).transpose(3, 1, 0, 2, 4).reshape(512, 32)
    return mixed_out, new_state.reshape(state.shape)


def solution(mesh):
    in_specs = (
        P("dp", ("kv", "tp")),
        P(("dp", "kv", "tp")),
        P(("dp", "kv", "tp"), None, None, None),
        P(),
        P(None, "kv"),
        P(None, "kv"),
        P("kv", None),
        P(),
        P(None, ("kv", "tp")),
        P(None, ("kv", "tp")),
        P(None, ("kv", "tp")),
        P(None, ("kv", "tp")),
        P(),
        P(),
        P(),
        P(None, ("kv", "tp")),
        P(),
        P(None, "kv"),
        P(None, "kv"),
        P("kv", None),
    )
    out_specs = (P("dp", ("kv", "tp")), P(("dp", "kv", "tp"), None, None, None))
    return jax.shard_map(
        per_device, mesh=mesh, in_specs=in_specs, out_specs=out_specs, check_vma=False
    )
```

```python
import math

import jax
import jax.numpy as jnp
from jax import lax
from jax.experimental import pallas as pl
from jax.experimental.pallas import tpu as pltpu
from jax.sharding import PartitionSpec as P

HEADS = 16
HEAD = 128
BLK = 8
D = 2048
NX = 4
NZ = 8
CHIPS = NX * NZ
ROWS = CHIPS * BLK
EPSILON = 1e-06
F32 = jnp.float32
BF16 = jnp.bfloat16
HIGH = lax.Precision.HIGHEST


def lanes_swapped(tiles):
    rows = tiles[0].shape[0]
    lane = lax.broadcasted_iota(jnp.int32, (rows, 128), 1)
    out = list(tiles)
    for step in (2, 1):
        width = step * 32
        low = (lane & width) == 0
        for i in range(4):
            if i & step:
                continue
            a, b = out[i], out[i + step]
            out[i] = jnp.where(low, a, pltpu.roll(b, width, 1))
            out[i + step] = jnp.where(low, pltpu.roll(a, 128 - width, 1), b)
    return out


def dot_nt(a, b, precision=None):
    return lax.dot_general(
        a, b, (((1,), (1,)), ((), ())), precision=precision, preferred_element_type=F32
    )


def wrapped(dz):
    return (dz + 3) % NZ - 3


def place(dx, dz):
    return (dx % NX) * NZ + dz % NZ


def children(half, dx, dz):
    dx, dz = dx % NX, wrapped(dz)
    if abs(dz) == 1:
        return []
    found = []
    if dx == 0:
        if dz == 0:
            found += [(0, 4)]
        if half == 0:
            found += [(2, dz)]
        found += [(-1, dz), (1, dz)]
        if dz == 0:
            found += [(0, 2), (0, -2), (0, 3), (0, -3), (0, 1), (0, -1)]
    else:
        if half == 1 and dx == NX - 1:
            found += [(2, dz)]
        if dz == 0:
            found += [(dx, 1), (dx, -1)]
    return found


GATHER_STEPS = (
    ("side", 0), ("column", 2), ("column", -2), ("far", 0), ("column", 3), ("column", -3), ("column", 4),
    ("relay", 2), ("row", 0), ("relay", -2), ("relay", 3), ("row", 1), ("relay", -3), ("relay", 4),
    ("row", -1), ("row", 2), ("row", -2), ("row", 3), ("row", -3), ("row", 4),
)
SUM_STEPS = (
    ("produce", 4), ("produce", 1), ("produce", -1), ("produce", 3), ("produce", -3),
    ("produce", 2), ("produce", -2), ("produce", 0),
    ("relay", 4), ("relay", 3), ("relay", -3), ("cross_row", 0), ("relay", 2), ("column", 4),
    ("relay", -2), ("column", 3), ("column", -3), ("relay", 0), ("column", 2), ("column", -2), ("column", 0),
)


class Torus:
    def __init__(self):
        self.kv = lax.axis_index("kv")
        self.tp = lax.axis_index("tp")
        self.x = lax.rem(self.kv, NX)
        self.z = lax.div(self.kv, NX)

    def at(self, dx, dz):
        return lax.rem(self.z + dz % NZ, NZ) * NX + lax.rem(self.x + dx % NX, NX)


def send(src, dst, send_sem, recv_sem, target):
    pltpu.make_async_remote_copy(
        src_ref=src,
        dst_ref=dst,
        send_sem=send_sem,
        recv_sem=recv_sem,
        device_id=target,
        device_id_type=pl.DeviceIdType.MESH,
    ).start()


def arrived(ref, sem):
    pltpu.make_async_copy(ref, ref, sem).wait()


def gather(torus, buf, send_sem, recv_sem, consume=None):
    def pass_on(half, dx, dz):
        source = torus.at(-dx, -dz)
        for cx, cz in children(half, dx, dz):
            send(
                buf.at[source, half],
                buf.at[source, half],
                send_sem,
                recv_sem.at[half, place(cx, cz)],
                {"kv": torus.at(cx - dx, cz - dz)},
            )

    def take(half, dx, dz):
        arrived(buf.at[torus.at(-dx, -dz), half], recv_sem.at[half, place(dx, dz)])
        pass_on(half, dx, dz)

    for half in range(2):
        pass_on(half, 0, 0)
    for what, dz in GATHER_STEPS:
        if what == "column":
            take(0, 0, dz)
            take(1, 0, dz)
        elif what == "side":
            for dx in (1, -1):
                take(0, dx, 0)
                take(1, dx, 0)
        elif what == "far":
            take(0, 2, 0)
            take(1, 2, 0)
        elif what == "relay":
            take(1, -1, dz)
        else:
            if abs(dz) == 1:
                places = [(half, dx) for dx in (0, 1, -1, 2) for half in range(2)]
            elif dz != 0:
                places = [(0, -1), (0, 1), (1, 1), (0, 2), (1, 2)]
            else:
                places = []
            for half, dx in places:
                take(half, dx, dz)
            if consume is not None:
                consume(lax.rem(torus.z + (-dz) % NZ, NZ))


def sum_at_owner(
    torus, part, relay, column, final, along_z, stage_x, stage_z, stage_row, send_sem, recv_sem, produce
):
    sums = [None, None]

    def slot(dz):
        return dz % NZ

    def z_slot(dx, dz):
        return (dx % NX) + (0 if dz == 1 else NX)

    def term(half, dx, dz):
        total = part[torus.at(-dx, -dz), half].astype(F32)
        if dz == 0 and dx != 0:
            for side in (1, -1):
                total = total + along_z[half, z_slot(dx, side)].astype(F32)
        return total

    def post(src, dst, half, place_at, target):
        send(src, dst, send_sem, recv_sem.at[half, place_at], {"kv": target})

    def produce_step(dz):
        produce(lax.rem(torus.z + (-dz) % NZ, NZ))
        for half in range(2):
            if abs(dz) == 1:
                for dx in (2, 1, -1):
                    n = z_slot(dx, dz)
                    post(part.at[torus.at(-dx, -dz), half], along_z.at[half, n], half, 32 + n, torus.at(0, -dz))
                post(
                    part.at[torus.at(0, -dz), half], final.at[half, slot(dz)], half, 24 + slot(dz), torus.at(0, -dz)
                )
            elif dz != 0:
                for dx in (2, 1, -1):
                    to_column(half, dx, dz, part.at[torus.at(-dx, -dz), half])

    def to_column(half, dx, dz, src):
        if half == 1 and dx == 2:
            post(src, relay.at[slot(dz)], half, slot(dz), torus.at(1, 0))
        elif half == 0 or dx == 1:
            n = {2: 2, 1: 0, -1: 1}[dx]
            post(src, column.at[half, n, slot(dz)], half, (8, 16, 0)[n] + slot(dz), torus.at(-dx, 0))

    def cross_row_step():
        for half in range(2):
            for dx in (2, 1, -1):
                for side in (1, -1):
                    n = z_slot(dx, side)
                    arrived(along_z.at[half, n], recv_sem.at[half, 32 + n])
        for half, dx in ((1, 2), (0, 2), (0, 1), (0, -1), (1, 1)):
            stage_row[half, dx % NX] = term(half, dx, 0).astype(BF16)
            to_column(half, dx, 0, stage_row.at[half, dx % NX])

    def relay_step(dz):
        arrived(relay.at[slot(dz)], recv_sem.at[1, slot(dz)])
        total = term(1, -1, dz) + relay[slot(dz)].astype(F32)
        stage_x[slot(dz)] = total.astype(BF16)
        post(stage_x.at[slot(dz)], column.at[1, 1, slot(dz)], 1, 16 + slot(dz), torus.at(1, 0))

    def column_step(half, dz):
        total = term(half, 0, dz)
        for n in range(3 - half):
            arrived(column.at[half, n, slot(dz)], recv_sem.at[half, (8, 16, 0)[n] + slot(dz)])
            total = total + column[half, n, slot(dz)].astype(F32)
        if dz == 0:
            sums[half] = total
            return
        stage_z[half, slot(dz)] = total.astype(BF16)
        post(stage_z.at[half, slot(dz)], final.at[half, slot(dz)], half, 24 + slot(dz), torus.at(0, -dz))

    for what, dz in SUM_STEPS:
        if what == "produce":
            produce_step(dz)
        elif what == "cross_row":
            cross_row_step()
        elif what == "relay":
            relay_step(dz)
        else:
            column_step(0, dz)
            column_step(1, dz)
    for dz in (1, -1, 4, 3, -3, 2, -2):
        for half in range(2):
            arrived(final.at[half, slot(dz)], recv_sem.at[half, 24 + slot(dz)])
            sums[half] = sums[half] + final[half, slot(dz)].astype(F32)
    return sums


def renew(h, state, fresh, update_refs):
    rows = slice(8 * h, 8 * h + 8)
    faded_ref, update_ref, kept_ref = update_refs
    gained = lax.dot_general(
        faded_ref[rows], update_ref[rows], (((0,), (0,)), ((), ())), precision=HIGH, preferred_element_type=F32
    )
    fresh[h] = kept_ref[8 * h : 8 * h + 1, :] * state[h] + gained


def unpack_row(buf, gain_ref, scaled_ref, squares_ref, zt):
    for tile in range(2):
        gain = gain_ref[:, pl.ds(pl.multiple_of(zt * 256 + 128 * tile, 128), 128)]
        for odd in range(2):
            for half in range(2):
                rows = slice(128 * odd + 64 * half, 128 * odd + 64 * half + 64)
                value = buf[4 * zt + 2 * tile + odd, half].astype(F32)
                scaled_ref[rows, 128 * tile : 128 * tile + 128] = (value * gain).astype(BF16)
                squares_ref[rows, :] += value * value


def scale_of(squares_ref):
    return lax.rsqrt(jnp.sum(squares_ref[...], axis=1, keepdims=True) / D + EPSILON)


def half_step(torus, buf, gain_ref, gate_ref, up_ref, down_ref, weight_waits, scaled_ref, squares_ref,
              acts, part, sum_refs, gather_sems, sum_sems, gathered=None):
    gate_act, up_act = acts
    squares_ref[...] = jnp.zeros_like(squares_ref)
    gate_act[...] = jnp.zeros_like(gate_act)
    up_act[...] = jnp.zeros_like(up_act)
    for wait in weight_waits:
        wait()

    def consume(zt):
        unpack_row(buf, gain_ref, scaled_ref, squares_ref, zt)
        channels = pl.ds(pl.multiple_of(zt * 256, 256), 256)
        scaled = scaled_ref[...]
        gate_act[...] += dot_nt(scaled, gate_ref[:, channels])
        up_act[...] += dot_nt(scaled, up_ref[:, channels])

    with jax.named_scope("gather"):
        gather(torus, buf, *gather_sems, consume)
    if gathered is not None:
        gathered()
    with jax.named_scope("units"):
        row_scale = scale_of(squares_ref)
        hidden = (jax.nn.silu(gate_act[...] * row_scale) * (up_act[...] * row_scale)).astype(BF16)

    def produce(zt):
        cols = pl.ds(pl.multiple_of(zt * 256, 256), 256)
        product = jnp.dot(hidden, down_ref[:, cols], preferred_element_type=F32)
        for tile in range(2):
            for odd in range(2):
                for half in range(2):
                    row = 128 * odd + 64 * half
                    block = product[row : row + 64, 128 * tile : 128 * tile + 128]
                    part[4 * zt + 2 * tile + odd, half] = block.astype(BF16)

    with jax.named_scope("sum"):
        return sum_at_owner(torus, part, *sum_refs, *sum_sems, produce)


def spread(rows):
    parts = [jnp.broadcast_to(rows[:, h : h + 1], (BLK, 128)) for h in range(HEADS)]
    return jnp.concatenate(parts, axis=0)


def delta(owned, write_pre, forget_pre, rates, live, state, update_refs):
    query, key, value, gating = owned
    live_heads = live[:, :HEADS]
    write = spread(jax.nn.sigmoid(write_pre) * live_heads)
    forget = spread(-jnp.exp(rates) * jax.nn.softplus(forget_pre) * live_heads)
    query_unit = query * lax.rsqrt(jnp.sum(query * query, axis=1, keepdims=True) + EPSILON)
    query_unit = query_unit / math.sqrt(HEAD)
    key_unit = key * lax.rsqrt(jnp.sum(key * key, axis=1, keepdims=True) + EPSILON)
    row = lax.broadcasted_iota(jnp.int32, (128, 128), 0)
    col = lax.broadcasted_iota(jnp.int32, (128, 128), 1)
    same = (row >> 3) == (col >> 3)
    causal = same & (col <= row)
    strict = same & (col < row)
    identity = jnp.where(row == col, 1.0, 0.0)

    def dot(a, b):
        return jnp.dot(a, b, precision=HIGH, preferred_element_type=F32)

    cumulative = dot(jnp.where(causal, 1.0, 0.0), forget)
    decay = jnp.where(causal, jnp.exp(jnp.minimum(cumulative - cumulative.T, 0.0)), 0.0)
    strict_part = jnp.where(strict, write * decay * dot_nt(key_unit, key_unit, HIGH), 0.0)
    squared = dot(strict_part, strict_part)
    fourth = dot(squared, squared)
    inverse = dot(dot(identity - strict_part, identity + squared), identity + fourth)
    growth = jnp.exp(cumulative)
    target = dot(inverse, write * value)
    key_mix = dot(inverse, write * growth * key_unit)
    scores = dot_nt(query_unit, key_unit, HIGH) * decay
    grown = query_unit * growth
    by_head = cumulative.reshape(HEADS, BLK, 128)
    last = by_head[:, BLK - 1 : BLK, :]
    fading = jnp.exp(last - by_head).reshape(128, 128)
    faded = key_unit * fading
    kept = jnp.exp(last)
    updates, reads = [], []
    for h in range(HEADS):
        rows = slice(8 * h, 8 * h + 8)
        both = jnp.concatenate([key_mix[rows], grown[rows]], axis=0)
        seen = dot(both, state[h])
        updates.append(target[rows] - seen[:BLK])
        reads.append(seen[BLK:])
    update = jnp.concatenate(updates, axis=0)
    faded_ref, update_ref, kept_ref = update_refs
    faded_ref[...] = faded
    update_ref[...] = update
    kept_ref[...] = jnp.broadcast_to(kept, (HEADS, BLK, 128)).reshape(128, 128)
    attend = jnp.concatenate(reads, axis=0) + dot(scores, update)
    normed = attend * lax.rsqrt(jnp.mean(attend * attend, axis=1, keepdims=True) + EPSILON)
    return normed * jax.nn.silu(gating) * jnp.concatenate([live] * HEADS, axis=0)


def layer(
    length, tokens, rates, gain_first, gain_mix, gain_second,
    gate1, up1, down1, gate2, up2, down2, query, key, value, gating, outw, writew, forgetw, state,
    out, new_state,
    buf_a, buf_c, buf_m, buf_g, scaled, squares, gate_act, up_act, project, part1, part2,
    relay1, column1, final1, along1, stage_x1, stage_z1, stage_row1,
    relay2, column2, final2, along2, stage_x2, stage_z2, stage_row2,
    v_gate1, v_up1, v_down1, v_gate2, v_up2, v_down2, v_all, v_out, v_state, v_fresh, faded_s, update_s, kept_s,
    s_length, outgoing, incoming, gates, tok, tok_in, last_stage, last_in,
    local_sem, send_sem, recv_ag, recv_rs, recv_x, pair_sem, quad_send, quad_recv,
):
    torus = Torus()
    update_refs = (faded_s, update_s, kept_s)

    def own_columns(t):
        return pl.multiple_of(128 * t, 128)

    kv, tp = torus.kv, torus.tp
    other = 1 - tp
    odd = lax.rem(kv, 2)
    twin = kv + 1 - 2 * odd
    seat = 2 * odd + tp
    own_out = pl.ds(pl.multiple_of(32 * seat, 32), 32)
    quad = [
        ({"tp": other}, 2 * odd + other),
        ({"kv": twin}, 2 * (1 - odd) + tp),
        ({"kv": twin, "tp": other}, 2 * (1 - odd) + other),
    ]

    with jax.named_scope("entry"):
        barrier = pltpu.get_barrier_semaphore()
        near = [{"kv": torus.at(dx, 0)} for dx in (1, -1, 2)]
        near += [{"kv": torus.at(0, dz)} for dz in (1, -1, 2, -2, 3, -3, 4)]
        near += [{"tp": other}, {"kv": twin, "tp": other}]
        for target in near:
            pl.semaphore_signal(barrier, inc=1, device_id=target, device_id_type=pl.DeviceIdType.MESH)
        loads = {}
        for n, (name, src, dst) in enumerate(
            [
                ("gate1", gate1, v_gate1), ("up1", up1, v_up1), ("down1", down1, v_down1),
                ("query", query, v_all.at[pl.ds(own_columns(tp), 32)]),
                ("key", key, v_all.at[pl.ds(own_columns(tp) + 32, 32)]),
                ("value", value, v_all.at[pl.ds(own_columns(tp) + 64, 32)]),
                ("gating", gating, v_all.at[pl.ds(own_columns(tp) + 96, 32)]),
                ("out", outw, v_out.at[own_out]),
                ("write", writew, v_all.at[256:272]), ("forget", forgetw, v_all.at[272:288]),
                ("state", state, v_state),
                ("length", length, s_length), ("gate2", gate2, v_gate2), ("up2", up2, v_up2), ("down2", down2, v_down2),
            ]
        ):
            loads[name] = pltpu.make_async_copy(src, dst, local_sem.at[n])
            loads[name].start()

        values = tokens[...].astype(F32)
        values = jnp.concatenate([values[:, 128 * q : 128 * q + 128] for q in range(4)], axis=0).T
        values = values.reshape(8, 2, BLK, 128)
        for parity in range(2):
            tok[parity] = values[:, parity].reshape(64, 128).astype(BF16)
        pl.semaphore_wait(barrier, len(near))
    with jax.named_scope("quad_in"):
        for n, (target, _) in enumerate(quad):
            row = tp if n == 1 else other
            send(tok.at[row], tok_in.at[seat], quad_send.at[n], quad_recv.at[seat], target)
        tok_in[seat] = tok[tp]
        for _, place_at in quad:
            arrived(tok_in.at[place_at], quad_recv.at[place_at])
        tiles = lanes_swapped([tok_in[j].astype(F32) for j in range(4)])
        for half in range(2):
            buf_a[kv, half] = jnp.where(odd == 0, tiles[half], tiles[2 + half]).astype(BF16)
    mine = v_all.at[pl.ds(own_columns(tp), 128)]

    def share_projections():
        for name in ("query", "key", "value", "gating"):
            loads[name].wait()
        loads["out"].wait()
        for n, (target, _) in enumerate(quad[:2]):
            send(v_out.at[own_out], v_out.at[own_out], quad_send.at[3 + n], quad_recv.at[4 + seat], target)
        send(mine, mine, pair_sem.at[0], pair_sem.at[1], {"tp": other})

    sums = half_step(
        torus, buf_a, gain_first, v_gate1, v_up1, v_down1,
        [loads["gate1"].wait, loads["up1"].wait, loads["down1"].wait],
        scaled, squares, (gate_act, up_act), part1,
        (relay1, column1, final1, along1, stage_x1, stage_z1, stage_row1),
        (send_sem.at[0], recv_ag.at[0]), (send_sem.at[1], recv_rs.at[0]), share_projections,
    )
    for half in range(2):
        buf_c[kv, half] = (buf_a[kv, half].astype(F32) + 0.5 * sums[half]).astype(BF16)

    arrived(v_all.at[pl.ds(own_columns(other), 128)], pair_sem.at[1])
    loads["write"].wait()
    loads["forget"].wait()
    squares[...] = jnp.zeros_like(squares)
    project[...] = jnp.zeros_like(project)

    def consume(zt):
        unpack_row(buf_c, gain_mix, scaled, squares, zt)
        channels = pl.ds(pl.multiple_of(zt * 256, 256), 256)
        project[...] += dot_nt(scaled[...], v_all[:, channels])

    with jax.named_scope("gather_c"):
        gather(torus, buf_c, send_sem.at[2], recv_ag.at[1], consume)
    with jax.named_scope("project"):
        mix_scale = scale_of(squares)
        for t in range(2):
            product = project[:, 128 * t : 128 * t + 128] * mix_scale
            outgoing[:, t] = product.reshape(CHIPS, BLK, 128).astype(BF16)
        gates[...] = project[:, 256:] * mix_scale
    with jax.named_scope("exchange"):
        for d in range(1, CHIPS):
            peer = lax.rem(kv + d, CHIPS)
            send(outgoing.at[peer], incoming.at[kv], send_sem.at[3], recv_x.at[d], {"kv": peer})
        incoming[kv] = outgoing[kv]
        own_rows = pl.ds(pl.multiple_of(kv * BLK, BLK), BLK)
        loads["length"].wait()
        position = lax.broadcasted_iota(jnp.int32, (BLK, 128), 0)
        live = jnp.where(position < s_length[0], 1.0, 0.0)
        loads["state"].wait()
        for d in range(1, CHIPS):
            arrived(incoming.at[lax.rem(kv + CHIPS - d, CHIPS)], recv_x.at[d])
    twin_seat = quad[1][1]
    twin_out = v_out.at[pl.ds(pl.multiple_of(32 * twin_seat, 32), 32)]
    with jax.named_scope("delta"):
        tiles = incoming[...].astype(F32).reshape(HEADS, 4, BLK, 128)
        owned = lanes_swapped([tiles[:, j].reshape(128, 128) for j in range(4)])
        gates_in = gates[own_rows, :]
        mixed = delta(owned, gates_in[:, :HEADS], gates_in[:, HEADS:], rates[...], live, v_state, update_refs)
        for h in range(HEADS):
            lanes = slice(128 * (h % 8), 128 * (h % 8) + 128)
            buf_m[kv, h // 8, :, lanes] = mixed[8 * h : 8 * h + 8].astype(BF16)
    heads_left = list(range(HEADS))

    def renew_two(zt):
        if len(heads_left) == HEADS:
            arrived(twin_out, quad_recv.at[4 + twin_seat])
            send(twin_out, twin_out, quad_send.at[5], quad_recv.at[4 + twin_seat], {"tp": other})
        for _ in range(2):
            renew(heads_left.pop(0), v_state, v_fresh, update_refs)

    with jax.named_scope("gather_m"):
        gather(torus, buf_m, send_sem.at[4], recv_ag.at[2], renew_two)
    save = pltpu.make_async_copy(v_fresh, new_state, local_sem.at[15])
    save.start()
    with jax.named_scope("out_product"):
        for place_at in (quad[0][1], quad[2][1]):
            rows = pl.ds(pl.multiple_of(32 * place_at, 32), 32)
            arrived(v_out.at[rows], quad_recv.at[4 + place_at])
        mixed_sum = jnp.zeros((128, 128), F32)
        for half in range(2):
            lanes = slice(half * (D // 2), (half + 1) * (D // 2))
            heads_half = buf_m[pl.ds(16 * odd, 16), half].astype(F32).reshape(128, D // 2).astype(BF16)
            mixed_sum = mixed_sum + dot_nt(heads_half, v_out[:, lanes]).astype(BF16).astype(F32)
        for half in range(2):
            rows = slice(64 * half, 64 * half + 64)
            buf_g[kv, half] = (buf_c[kv, half].astype(F32) + mixed_sum[rows]).astype(BF16)

    sums = half_step(
        torus, buf_g, gain_second, v_gate2, v_up2, v_down2,
        [loads["gate2"].wait, loads["up2"].wait, loads["down2"].wait],
        scaled, squares, (gate_act, up_act), part2,
        (relay2, column2, final2, along2, stage_x2, stage_z2, stage_row2),
        (send_sem.at[5], recv_ag.at[3]), (send_sem.at[6], recv_rs.at[1]),
    )
    with jax.named_scope("finish"):
        for half in range(2):
            last_stage[half] = (buf_g[kv, half].astype(F32) + 0.5 * sums[half]).astype(BF16)
        for n, (target, _) in enumerate(quad):
            send(last_stage, last_in.at[tp, odd], quad_send.at[6 + n], quad_recv.at[8 + 2 * odd + tp], target)
        last_in[tp, odd] = last_stage[...]
        for _, place_at in quad:
            from_odd, from_tp = lax.div(place_at, 2), lax.rem(place_at, 2)
            arrived(last_in.at[from_tp, from_odd], quad_recv.at[8 + place_at])
        sides = []
        for parity in range(2):
            tiles = [last_in[parity, q // 2, q % 2].astype(F32) for q in range(4)]
            tiles = lanes_swapped(tiles)
            low = jnp.where(tp == 0, tiles[0], tiles[1])
            high = jnp.where(tp == 0, tiles[2], tiles[3])
            sides.append(jnp.where(odd == 0, low, high).reshape(8, 1, BLK, 128))
        both = jnp.concatenate(sides, axis=1).reshape(128, 128).T.astype(BF16)
        for q in range(4):
            out[:, 128 * q : 128 * q + 128] = both[32 * q : 32 * q + 32]

        arrived(mine, pair_sem.at[0])
        for n, (target, _) in enumerate(quad):
            arrived(tok.at[tp if n == 1 else other], quad_send.at[n])
            arrived(v_out.at[own_out], quad_send.at[3 + n])
            arrived(last_stage, quad_send.at[6 + n])
        everything = pl.ds(0, CHIPS - 1)
        for n, ref in (
            (0, buf_a), (1, part1), (2, buf_c), (3, incoming), (4, buf_m), (5, buf_g), (6, part2)
        ):
            arrived(ref.at[everything], send_sem.at[n])
        save.wait()


def run_layer(*arrays):
    bf, fl = BF16, F32
    dma = pltpu.SemaphoreType.DMA
    whole = (CHIPS, 2, 64, 128)
    in_vmem = pl.BlockSpec(memory_space=pltpu.VMEM)
    in_hbm = pl.BlockSpec(memory_space=pl.ANY)
    ff = 176
    eight = (8, 64, 128)
    sum_set = [
        pltpu.VMEM(eight, bf), pltpu.VMEM((2, 3, *eight), bf), pltpu.VMEM((2, *eight), bf), pltpu.VMEM((2, *eight), bf),
        pltpu.VMEM(eight, bf), pltpu.VMEM((2, *eight), bf), pltpu.VMEM((2, 4, 64, 128), bf),
    ]
    return pl.pallas_call(
        layer,
        out_shape=(
            jax.ShapeDtypeStruct((32, 512), bf),
            jax.ShapeDtypeStruct((HEADS, HEAD, HEAD), fl),
        ),
        in_specs=[in_hbm] + [in_vmem] * 5 + [in_hbm] * 14,
        out_specs=(in_vmem, in_hbm),
        scratch_shapes=[
            pltpu.VMEM(whole, bf), pltpu.VMEM(whole, bf),
            pltpu.VMEM((CHIPS, 2, BLK, D // 2), bf), pltpu.VMEM(whole, bf),
            pltpu.VMEM((ROWS, 256), bf), pltpu.VMEM((ROWS, 128), fl),
            pltpu.VMEM((ROWS, ff), fl), pltpu.VMEM((ROWS, ff), fl), pltpu.VMEM((ROWS, 256 + 2 * HEADS), fl),
            pltpu.VMEM(whole, bf), pltpu.VMEM(whole, bf),
            *sum_set, *sum_set,
            *([pltpu.VMEM((ff, D), bf)] * 6),
            pltpu.VMEM((256 + 2 * HEADS, D), bf), pltpu.VMEM((128, D), bf),
            *([pltpu.VMEM((HEADS, HEAD, HEAD), fl)] * 2), *([pltpu.VMEM((128, 128), fl)] * 3),
            pltpu.SMEM((1,), jnp.int32), pltpu.VMEM((CHIPS, 2, BLK, 128), bf), pltpu.VMEM((CHIPS, 2, BLK, 128), bf),
            pltpu.VMEM((ROWS, 2 * HEADS), fl), pltpu.VMEM((2, 64, 128), bf), pltpu.VMEM((4, 64, 128), bf),
            pltpu.VMEM((2, 64, 128), bf), pltpu.VMEM((2, 2, 2, 64, 128), bf),
            dma((16,)), dma((7,)), dma((4, 2, 32)), dma((2, 2, 40)), dma((32,)), dma((2,)), dma((9,)), dma((12,)),
        ],
        compiler_params=pltpu.CompilerParams(
            collective_id=0, has_side_effects=True, vmem_limit_bytes=60_000_000
        ),
        name="layer",
    )(*arrays)


def store(out, state, out_hbm, state_hbm, out_vmem, state_vmem, sems):
    pieces = [(out, out_vmem, out_hbm)]
    for n in range(4):
        heads = pl.ds(4 * n, 4)
        pieces.append((state.at[heads], state_vmem.at[heads], state_hbm.at[heads]))
    reads = [pltpu.make_async_copy(a, b, sems.at[0, n]) for n, (a, b, _) in enumerate(pieces)]
    writes = [pltpu.make_async_copy(b, c, sems.at[1, n]) for n, (_, b, c) in enumerate(pieces)]
    for read in reads:
        read.start()
    for read, write in zip(reads, writes):
        read.wait()
        write.start()
    for write in writes:
        write.wait()


def stored(out, state):
    anywhere = pl.BlockSpec(memory_space=pl.ANY)
    return pl.pallas_call(
        store,
        out_shape=(jax.ShapeDtypeStruct(out.shape, out.dtype), jax.ShapeDtypeStruct(state.shape, state.dtype)),
        in_specs=[anywhere] * 2,
        out_specs=(anywhere,) * 2,
        scratch_shapes=[
            pltpu.VMEM(out.shape, out.dtype), pltpu.VMEM(state.shape, state.dtype), pltpu.SemaphoreType.DMA((2, 5)),
        ],
        compiler_params=pltpu.CompilerParams(vmem_limit_bytes=60_000_000),
        name="store",
    )(out, state)


def per_device(
    tokens,
    lengths,
    state,
    gain_first,
    first_gate,
    first_up,
    first_down,
    gain_mix,
    query_weight,
    key_weight,
    value_weight,
    gating_weight,
    write_weight,
    forget_weight,
    forget_rate,
    out_weight,
    gain_second,
    second_gate,
    second_up,
    second_down,
):
    out, new_state = run_layer(
        lengths, tokens.T, forget_rate[None, :], gain_first[None, :], gain_mix[None, :], gain_second[None, :],
        first_gate.T, first_up.T, first_down, second_gate.T, second_up.T, second_down,
        query_weight.T, key_weight.T, value_weight.T, gating_weight.T, out_weight.T,
        write_weight.T, forget_weight.T, state.reshape(HEADS, HEAD, HEAD),
    )
    out, new_state = stored(out, new_state)
    return out.T, new_state.reshape(state.shape)


def solution(mesh):
    in_specs = (
        P("dp", ("kv", "tp")),
        P(("dp", "kv", "tp")),
        P(("dp", "kv", "tp"), None, None, None),
        P(),
        P(None, "kv"),
        P(None, "kv"),
        P("kv", None),
        P(),
        P(None, ("kv", "tp")),
        P(None, ("kv", "tp")),
        P(None, ("kv", "tp")),
        P(None, ("kv", "tp")),
        P(),
        P(),
        P(),
        P(None, ("kv", "tp")),
        P(),
        P(None, "kv"),
        P(None, "kv"),
        P("kv", None),
    )
    out_specs = (P("dp", ("kv", "tp")), P(("dp", "kv", "tp"), None, None, None))
    return jax.shard_map(
        per_device, mesh=mesh, in_specs=in_specs, out_specs=out_specs, check_vma=False
    )
```

```python
import math

import jax
import jax.numpy as jnp
from jax import lax
from jax.experimental import pallas as pl
from jax.experimental.pallas import tpu as pltpu
from jax.sharding import PartitionSpec as P

HEADS = 16
HEAD = 128
BLK = 8
D = 2048
NX = 4
NZ = 8
CHIPS = NX * NZ
ROWS = CHIPS * BLK
EPSILON = 1e-06
F32 = jnp.float32
BF16 = jnp.bfloat16
HIGH = lax.Precision.HIGHEST


def lanes_swapped(tiles):
    rows = tiles[0].shape[0]
    lane = lax.broadcasted_iota(jnp.int32, (rows, 128), 1)
    out = list(tiles)
    for step in (2, 1):
        width = step * 32
        low = (lane & width) == 0
        for i in range(4):
            if i & step:
                continue
            a, b = out[i], out[i + step]
            out[i] = jnp.where(low, a, pltpu.roll(b, width, 1))
            out[i + step] = jnp.where(low, pltpu.roll(a, 128 - width, 1), b)
    return out


def dot_nt(a, b, precision=None):
    return lax.dot_general(
        a, b, (((1,), (1,)), ((), ())), precision=precision, preferred_element_type=F32
    )


def wrapped(dz):
    return (dz + 3) % NZ - 3


def place(dx, dz):
    return (dx % NX) * NZ + dz % NZ


def children(half, dx, dz):
    sign = 1 if half == 0 else -1
    dx, dz = dx % NX, wrapped(dz)
    if abs(dz) == 1:
        return []
    found = []
    if dx == 0:
        found += [(sign, dz), (-sign, dz)]
        if dz == 0:
            found += [(0, 2), (0, -2), (0, 3), (0, -3), (0, 4), (0, 1), (0, -1)]
    else:
        if dx == sign % NX:
            found += [(2, dz)]
        if dz == 0:
            found += [(dx, 1), (dx, -1)]
    return found


GATHER_STEPS = (
    ("side", 0), ("column", 2), ("column", -2), ("far", 0), ("column", 3), ("column", -3), ("column", 4),
    ("relay", 2), ("row", 0), ("relay", -2), ("relay", 3), ("row", 1), ("relay", -3), ("relay", 4),
    ("row", -1), ("row", 2), ("row", -2), ("row", 3), ("row", -3), ("row", 4),
)
SUM_STEPS = (
    ("produce", 4), ("produce", 1), ("produce", -1), ("produce", 3), ("produce", -3),
    ("produce", 2), ("produce", -2), ("produce", 0),
    ("relay", 4), ("relay", 3), ("relay", -3), ("cross_row", 0), ("relay", 2), ("column", 4),
    ("relay", -2), ("column", 3), ("column", -3), ("relay", 0), ("column", 2), ("column", -2), ("column", 0),
)


class Torus:
    def __init__(self):
        self.kv = lax.axis_index("kv")
        self.tp = lax.axis_index("tp")
        self.x = lax.rem(self.kv, NX)
        self.z = lax.div(self.kv, NX)

    def at(self, dx, dz):
        return lax.rem(self.z + dz % NZ, NZ) * NX + lax.rem(self.x + dx % NX, NX)


def send(src, dst, send_sem, recv_sem, target):
    pltpu.make_async_remote_copy(
        src_ref=src,
        dst_ref=dst,
        send_sem=send_sem,
        recv_sem=recv_sem,
        device_id=target,
        device_id_type=pl.DeviceIdType.MESH,
    ).start()


def arrived(ref, sem):
    pltpu.make_async_copy(ref, ref, sem).wait()


def gather(torus, buf, send_sem, recv_sem, consume=None, started=None):
    def pass_on(half, dx, dz, only=None):
        source = torus.at(-dx, -dz)
        targets = children(half, dx, dz)
        for cx, cz in targets if only is None else targets[only : only + 1]:
            send(
                buf.at[source, half],
                buf.at[source, half],
                send_sem,
                recv_sem.at[half, place(cx, cz)],
                {"kv": torus.at(cx - dx, cz - dz)},
            )

    def take(half, dx, dz):
        arrived(buf.at[torus.at(-dx, -dz), half], recv_sem.at[half, place(dx, dz)])
        pass_on(half, dx, dz)

    for hop in range(len(children(0, 0, 0))):
        for half in range(2):
            pass_on(half, 0, 0, hop)
    if started is not None:
        started()
    for what, dz in GATHER_STEPS:
        if what == "column":
            take(0, 0, dz)
            take(1, 0, dz)
        elif what == "side":
            for dx in (1, -1):
                take(0, dx, 0)
                take(1, dx, 0)
        elif what == "far":
            take(0, 2, 0)
            take(1, 2, 0)
        elif what == "relay":
            take(0, 1, dz)
            take(1, -1, dz)
        else:
            if abs(dz) == 1:
                places = [(half, dx) for dx in (0, 1, -1, 2) for half in range(2)]
            elif dz != 0:
                places = [(0, -1), (1, 1), (0, 2), (1, 2)]
            else:
                places = []
            for half, dx in places:
                take(half, dx, dz)
            if consume is not None:
                consume(lax.rem(torus.z + (-dz) % NZ, NZ))


def sum_at_owner(
    torus, part, relay, column, final, along_z, stage_x, stage_z, stage_row, send_sem, recv_sem, produce
):
    sums = [None, None]

    def slot(dz):
        return dz % NZ

    def z_slot(dx, dz):
        return (dx % NX) + (0 if dz == 1 else NX)

    def term(half, dx, dz):
        total = part[torus.at(-dx, -dz), half].astype(F32)
        if dz == 0 and dx != 0:
            for side in (1, -1):
                total = total + along_z[half, z_slot(dx, side)].astype(F32)
        return total

    def post(src, dst, half, place_at, target):
        send(src, dst, send_sem, recv_sem.at[half, place_at], {"kv": target})

    def produce_step(dz):
        produce(lax.rem(torus.z + (-dz) % NZ, NZ))
        for half in range(2):
            if abs(dz) == 1:
                for dx in (2, 1, -1):
                    n = z_slot(dx, dz)
                    post(part.at[torus.at(-dx, -dz), half], along_z.at[half, n], half, 32 + n, torus.at(0, -dz))
                post(
                    part.at[torus.at(0, -dz), half], final.at[half, slot(dz)], half, 24 + slot(dz), torus.at(0, -dz)
                )
            elif dz != 0:
                for dx in (2, 1, -1):
                    to_column(half, dx, dz, part.at[torus.at(-dx, -dz), half])

    def to_column(half, dx, dz, src):
        sign = 1 if half == 0 else -1
        if dx == 2:
            post(src, relay.at[half, slot(dz)], half, slot(dz), torus.at(-sign, 0))
        elif dx == -sign:
            post(src, column.at[half, 0, slot(dz)], half, 8 + slot(dz), torus.at(sign, 0))

    def cross_row_step():
        for half in range(2):
            for dx in (2, 1, -1):
                for side in (1, -1):
                    n = z_slot(dx, side)
                    arrived(along_z.at[half, n], recv_sem.at[half, 32 + n])
        for half, dx in ((0, 2), (1, 2), (0, -1), (1, 1)):
            stage_row[half, dx % NX] = term(half, dx, 0).astype(BF16)
            to_column(half, dx, 0, stage_row.at[half, dx % NX])

    def relay_step(half, dz):
        sign = 1 if half == 0 else -1
        arrived(relay.at[half, slot(dz)], recv_sem.at[half, slot(dz)])
        total = term(half, sign, dz) + relay[half, slot(dz)].astype(F32)
        stage_x[half, slot(dz)] = total.astype(BF16)
        post(stage_x.at[half, slot(dz)], column.at[half, 1, slot(dz)], half, 16 + slot(dz), torus.at(-sign, 0))

    def column_step(half, dz):
        total = term(half, 0, dz)
        for n in range(2):
            arrived(column.at[half, n, slot(dz)], recv_sem.at[half, 8 + 8 * n + slot(dz)])
            total = total + column[half, n, slot(dz)].astype(F32)
        if dz == 0:
            sums[half] = total
            return
        stage_z[half, slot(dz)] = total.astype(BF16)
        post(stage_z.at[half, slot(dz)], final.at[half, slot(dz)], half, 24 + slot(dz), torus.at(0, -dz))

    for what, dz in SUM_STEPS:
        if what == "produce":
            produce_step(dz)
        elif what == "cross_row":
            cross_row_step()
        elif what == "relay":
            relay_step(0, dz)
            relay_step(1, dz)
        else:
            column_step(0, dz)
            column_step(1, dz)
    for dz in (1, -1, 4, 3, -3, 2, -2):
        for half in range(2):
            arrived(final.at[half, slot(dz)], recv_sem.at[half, 24 + slot(dz)])
            sums[half] = sums[half] + final[half, slot(dz)].astype(F32)
    return sums


def renew(h, state, fresh, update_refs):
    rows = slice(8 * h, 8 * h + 8)
    faded_ref, update_ref, kept_ref = update_refs
    gained = lax.dot_general(
        faded_ref[rows], update_ref[rows], (((0,), (0,)), ((), ())), precision=HIGH, preferred_element_type=F32
    )
    fresh[h] = kept_ref[8 * h : 8 * h + 1, :] * state[h] + gained


def unpack_row(buf, gain_ref, scaled_ref, squares_ref, zt):
    for tile in range(2):
        gain = gain_ref[:, pl.ds(pl.multiple_of(zt * 256 + 128 * tile, 128), 128)]
        for odd in range(2):
            for half in range(2):
                rows = slice(128 * odd + 64 * half, 128 * odd + 64 * half + 64)
                value = buf[4 * zt + 2 * tile + odd, half].astype(F32)
                scaled_ref[rows, 128 * tile : 128 * tile + 128] = (value * gain).astype(BF16)
                squares_ref[rows, :] += value * value


def scale_of(squares_ref):
    return lax.rsqrt(jnp.sum(squares_ref[...], axis=1, keepdims=True) / D + EPSILON)


def half_step(torus, buf, gain_ref, gate_ref, up_ref, down_ref, weight_waits, scaled_ref, squares_ref,
              acts, part, sum_refs, gather_sems, sum_sems, started=None, gathered=None):
    gate_act, up_act = acts
    squares_ref[...] = jnp.zeros_like(squares_ref)
    gate_act[...] = jnp.zeros_like(gate_act)
    up_act[...] = jnp.zeros_like(up_act)
    for wait in weight_waits:
        wait()

    def consume(zt):
        unpack_row(buf, gain_ref, scaled_ref, squares_ref, zt)
        channels = pl.ds(pl.multiple_of(zt * 256, 256), 256)
        scaled = scaled_ref[...]
        gate_act[...] += dot_nt(scaled, gate_ref[:, channels])
        up_act[...] += dot_nt(scaled, up_ref[:, channels])

    with jax.named_scope("gather"):
        gather(torus, buf, *gather_sems, consume, started)
    if gathered is not None:
        gathered()
    with jax.named_scope("units"):
        row_scale = scale_of(squares_ref)
        hidden = (jax.nn.silu(gate_act[...] * row_scale) * (up_act[...] * row_scale)).astype(BF16)

    def produce(zt):
        cols = pl.ds(pl.multiple_of(zt * 256, 256), 256)
        product = jnp.dot(hidden, down_ref[:, cols], preferred_element_type=F32)
        for tile in range(2):
            for odd in range(2):
                for half in range(2):
                    row = 128 * odd + 64 * half
                    block = product[row : row + 64, 128 * tile : 128 * tile + 128]
                    part[4 * zt + 2 * tile + odd, half] = block.astype(BF16)

    with jax.named_scope("sum"):
        return sum_at_owner(torus, part, *sum_refs, *sum_sems, produce)


def spread(rows):
    parts = [jnp.broadcast_to(rows[:, h : h + 1], (BLK, 128)) for h in range(HEADS)]
    return jnp.concatenate(parts, axis=0)


def decays(write_pre, forget_pre, rates, live):
    live_heads = live[:, :HEADS]
    write = spread(jax.nn.sigmoid(write_pre) * live_heads)
    forget = spread(-jnp.exp(rates) * jax.nn.softplus(forget_pre) * live_heads)
    row = lax.broadcasted_iota(jnp.int32, (128, 128), 0)
    col = lax.broadcasted_iota(jnp.int32, (128, 128), 1)
    causal = ((row >> 3) == (col >> 3)) & (col <= row)
    cumulative = jnp.dot(
        jnp.where(causal, 1.0, 0.0), forget, precision=HIGH, preferred_element_type=F32
    )
    decay = jnp.where(causal, jnp.exp(jnp.minimum(cumulative - cumulative.T, 0.0)), 0.0)
    by_head = cumulative.reshape(HEADS, BLK, 128)
    last = by_head[:, BLK - 1 : BLK, :]
    fading = jnp.exp(last - by_head).reshape(128, 128)
    kept = jnp.broadcast_to(jnp.exp(last), (HEADS, BLK, 128)).reshape(128, 128)
    return write, jnp.exp(cumulative), decay, fading, kept


def delta(owned, decays_ref, live, state, update_refs):
    query, key, value, gating = owned
    write, growth, decay = decays_ref[0], decays_ref[1], decays_ref[2]
    query_unit = query * lax.rsqrt(jnp.sum(query * query, axis=1, keepdims=True) + EPSILON)
    query_unit = query_unit / math.sqrt(HEAD)
    key_unit = key * lax.rsqrt(jnp.sum(key * key, axis=1, keepdims=True) + EPSILON)
    row = lax.broadcasted_iota(jnp.int32, (128, 128), 0)
    col = lax.broadcasted_iota(jnp.int32, (128, 128), 1)
    strict = col < row
    identity = jnp.where(row == col, 1.0, 0.0)

    def dot(a, b):
        return jnp.dot(a, b, precision=HIGH, preferred_element_type=F32)

    strict_part = jnp.where(strict, write * decay * dot_nt(key_unit, key_unit, HIGH), 0.0)
    squared = dot(strict_part, strict_part)
    fourth = dot(squared, squared)
    inverse = dot(dot(identity - strict_part, identity + squared), identity + fourth)
    target = dot(inverse, write * value)
    key_mix = dot(inverse, write * growth * key_unit)
    scores = dot_nt(query_unit, key_unit, HIGH) * decay
    grown = query_unit * growth
    faded = key_unit * decays_ref[3]
    updates, reads = [], []
    for h in range(HEADS):
        rows = slice(8 * h, 8 * h + 8)
        both = jnp.concatenate([key_mix[rows], grown[rows]], axis=0)
        seen = dot(both, state[h])
        updates.append(target[rows] - seen[:BLK])
        reads.append(seen[BLK:])
    update = jnp.concatenate(updates, axis=0)
    faded_ref, update_ref, _ = update_refs
    faded_ref[...] = faded
    update_ref[...] = update
    attend = jnp.concatenate(reads, axis=0) + dot(scores, update)
    normed = attend * lax.rsqrt(jnp.mean(attend * attend, axis=1, keepdims=True) + EPSILON)
    return normed * jax.nn.silu(gating) * jnp.concatenate([live] * HEADS, axis=0)


def layer(
    length, tokens, rates, gain_first, gain_mix, gain_second,
    gate1, up1, down1, gate2, up2, down2, query, key, value, gating, outw, writew, forgetw, state,
    out, new_state,
    buf_a, buf_c, buf_m, buf_g, scaled, squares, gate_act, up_act, project, part1, part2,
    relay1, column1, final1, along1, stage_x1, stage_z1, stage_row1,
    relay2, column2, final2, along2, stage_x2, stage_z2, stage_row2,
    v_gate1, v_up1, v_down1, v_gate2, v_up2, v_down2, v_all, v_out, v_state, v_fresh, faded_s, update_s, decays_s,
    v_tokens, v_rates, v_gains, s_length, outgoing, incoming, gates, tok, tok_in, last_stage, last_in,
    local_sem, send_sem, recv_ag, recv_rs, recv_x, pair_sem, quad_send, quad_recv,
):
    torus = Torus()
    update_refs = (faded_s, update_s, decays_s.at[4])

    def own_columns(t):
        return pl.multiple_of(128 * t, 128)

    kv, tp = torus.kv, torus.tp
    other = 1 - tp
    odd = lax.rem(kv, 2)
    twin = kv + 1 - 2 * odd
    seat = 2 * odd + tp
    own_out = pl.ds(pl.multiple_of(32 * seat, 32), 32)
    quad = [
        ({"tp": other}, 2 * odd + other),
        ({"kv": twin}, 2 * (1 - odd) + tp),
        ({"kv": twin, "tp": other}, 2 * (1 - odd) + other),
    ]

    with jax.named_scope("entry"):
        barrier = pltpu.get_barrier_semaphore()
        near = [{"kv": torus.at(dx, 0)} for dx in (1, -1)]
        near += [{"kv": torus.at(0, dz)} for dz in (1, -1, 2, -2, 3, -3, 4)]
        near += [{"tp": other}, {"kv": twin, "tp": other}]
        for target in near:
            pl.semaphore_signal(barrier, inc=1, device_id=target, device_id_type=pl.DeviceIdType.MESH)
        loads = {}
        for n, (name, src, dst) in enumerate(
            [
                ("tokens", tokens, v_tokens), ("gain1", gain_first, v_gains.at[0]),
                ("gate1", gate1, v_gate1), ("up1", up1, v_up1), ("down1", down1, v_down1),
                ("query", query, v_all.at[pl.ds(own_columns(tp), 32)]),
                ("key", key, v_all.at[pl.ds(own_columns(tp) + 32, 32)]),
                ("value", value, v_all.at[pl.ds(own_columns(tp) + 64, 32)]),
                ("gating", gating, v_all.at[pl.ds(own_columns(tp) + 96, 32)]),
                ("out", outw, v_out.at[own_out]),
                ("write", writew, v_all.at[256:272]), ("forget", forgetw, v_all.at[272:288]),
                ("state", state, v_state),
                ("length", length, s_length), ("rates", rates, v_rates),
                ("gain_mix", gain_mix, v_gains.at[1]), ("gain2", gain_second, v_gains.at[2]),
                ("gate2", gate2, v_gate2), ("up2", up2, v_up2), ("down2", down2, v_down2),
            ]
        ):
            loads[name] = pltpu.make_async_copy(src, dst, local_sem.at[n])
            loads[name].start()

        loads["tokens"].wait()
        values = v_tokens[...].astype(F32)
        values = jnp.concatenate([values[:, 128 * q : 128 * q + 128] for q in range(4)], axis=0).T
        values = values.reshape(8, 2, BLK, 128)
        for parity in range(2):
            tok[parity] = values[:, parity].reshape(64, 128).astype(BF16)
        pl.semaphore_wait(barrier, len(near))
    with jax.named_scope("quad_in"):
        for n, (target, _) in enumerate(quad):
            row = tp if n == 1 else other
            send(tok.at[row], tok_in.at[seat], quad_send.at[n], quad_recv.at[seat], target)
        tok_in[seat] = tok[tp]
        for _, place_at in quad:
            arrived(tok_in.at[place_at], quad_recv.at[place_at])
        tiles = lanes_swapped([tok_in[j].astype(F32) for j in range(4)])
        for half in range(2):
            buf_a[kv, half] = jnp.where(odd == 0, tiles[half], tiles[2 + half]).astype(BF16)
    mine = v_all.at[pl.ds(own_columns(tp), 128)]

    def share_out():
        loads["out"].wait()
        send(v_out.at[own_out], v_out.at[own_out], quad_send.at[4], quad_recv.at[4 + seat], {"kv": twin})

    def share_projections():
        for name in ("query", "key", "value", "gating"):
            loads[name].wait()
        send(v_out.at[own_out], v_out.at[own_out], quad_send.at[3], quad_recv.at[4 + seat], {"tp": other})
        send(mine, mine, pair_sem.at[0], pair_sem.at[1], {"tp": other})

    sums = half_step(
        torus, buf_a, v_gains.at[0], v_gate1, v_up1, v_down1,
        [loads["gain1"].wait, loads["gate1"].wait, loads["up1"].wait, loads["down1"].wait],
        scaled, squares, (gate_act, up_act), part1,
        (relay1, column1, final1, along1, stage_x1, stage_z1, stage_row1),
        (send_sem.at[0], recv_ag.at[0]), (send_sem.at[1], recv_rs.at[0]), share_out, share_projections,
    )
    for half in range(2):
        buf_c[kv, half] = (buf_a[kv, half].astype(F32) + 0.5 * sums[half]).astype(BF16)

    arrived(v_all.at[pl.ds(own_columns(other), 128)], pair_sem.at[1])
    loads["write"].wait()
    loads["gain_mix"].wait()
    loads["forget"].wait()
    squares[...] = jnp.zeros_like(squares)
    project[...] = jnp.zeros_like(project)

    def consume(zt):
        unpack_row(buf_c, v_gains.at[1], scaled, squares, zt)
        channels = pl.ds(pl.multiple_of(zt * 256, 256), 256)
        project[...] += dot_nt(scaled[...], v_all[:, channels])

    with jax.named_scope("gather_c"):
        gather(torus, buf_c, send_sem.at[2], recv_ag.at[1], consume)
    with jax.named_scope("project"):
        mix_scale = scale_of(squares)
        for t in range(2):
            product = project[:, 128 * t : 128 * t + 128] * mix_scale
            outgoing[:, t] = product.reshape(CHIPS, BLK, 128).astype(BF16)
        gates[...] = project[:, 256:] * mix_scale
    with jax.named_scope("exchange"):
        for d in range(1, CHIPS):
            peer = lax.rem(kv + d, CHIPS)
            send(outgoing.at[peer], incoming.at[kv], send_sem.at[3], recv_x.at[d], {"kv": peer})
        incoming[kv] = outgoing[kv]
        own_rows = pl.ds(pl.multiple_of(kv * BLK, BLK), BLK)
        loads["length"].wait()
        position = lax.broadcasted_iota(jnp.int32, (BLK, 128), 0)
        live = jnp.where(position < s_length[0], 1.0, 0.0)
        loads["state"].wait()
        loads["rates"].wait()
        gates_in = gates[own_rows, :]
        for n, value in enumerate(decays(gates_in[:, :HEADS], gates_in[:, HEADS:], v_rates[...], live)):
            decays_s[n] = value
        for d in range(1, CHIPS):
            arrived(incoming.at[lax.rem(kv + CHIPS - d, CHIPS)], recv_x.at[d])
    twin_seat = quad[1][1]
    twin_out = v_out.at[pl.ds(pl.multiple_of(32 * twin_seat, 32), 32)]
    with jax.named_scope("delta"):
        tiles = incoming[...].astype(F32).reshape(HEADS, 4, BLK, 128)
        owned = lanes_swapped([tiles[:, j].reshape(128, 128) for j in range(4)])
        mixed = delta(owned, decays_s, live, v_state, update_refs)
        for h in range(HEADS):
            lanes = slice(128 * (h % 8), 128 * (h % 8) + 128)
            buf_m[kv, h // 8, :, lanes] = mixed[8 * h : 8 * h + 8].astype(BF16)
    heads_left = list(range(HEADS))

    def renew_two(zt):
        if len(heads_left) == HEADS:
            arrived(twin_out, quad_recv.at[4 + twin_seat])
            send(twin_out, twin_out, quad_send.at[5], quad_recv.at[4 + twin_seat], {"tp": other})
        for _ in range(2):
            renew(heads_left.pop(0), v_state, v_fresh, update_refs)

    with jax.named_scope("gather_m"):
        gather(torus, buf_m, send_sem.at[4], recv_ag.at[2], renew_two)
    save = pltpu.make_async_copy(v_fresh, new_state, local_sem.at[20])
    save.start()
    with jax.named_scope("out_product"):
        for place_at in (quad[0][1], quad[2][1]):
            rows = pl.ds(pl.multiple_of(32 * place_at, 32), 32)
            arrived(v_out.at[rows], quad_recv.at[4 + place_at])
        mixed_sum = jnp.zeros((128, 128), F32)
        for half in range(2):
            lanes = slice(half * (D // 2), (half + 1) * (D // 2))
            heads_half = buf_m[pl.ds(16 * odd, 16), half].astype(F32).reshape(128, D // 2).astype(BF16)
            mixed_sum = mixed_sum + dot_nt(heads_half, v_out[:, lanes]).astype(BF16).astype(F32)
        for half in range(2):
            rows = slice(64 * half, 64 * half + 64)
            buf_g[kv, half] = (buf_c[kv, half].astype(F32) + mixed_sum[rows]).astype(BF16)

    sums = half_step(
        torus, buf_g, v_gains.at[2], v_gate2, v_up2, v_down2,
        [loads["gain2"].wait, loads["gate2"].wait, loads["up2"].wait, loads["down2"].wait],
        scaled, squares, (gate_act, up_act), part2,
        (relay2, column2, final2, along2, stage_x2, stage_z2, stage_row2),
        (send_sem.at[5], recv_ag.at[3]), (send_sem.at[6], recv_rs.at[1]),
    )
    with jax.named_scope("finish"):
        for half in range(2):
            last_stage[half] = (buf_g[kv, half].astype(F32) + 0.5 * sums[half]).astype(BF16)
        for n, (target, _) in enumerate(quad):
            send(last_stage, last_in.at[tp, odd], quad_send.at[6 + n], quad_recv.at[8 + 2 * odd + tp], target)
        last_in[tp, odd] = last_stage[...]
        for _, place_at in quad:
            from_odd, from_tp = lax.div(place_at, 2), lax.rem(place_at, 2)
            arrived(last_in.at[from_tp, from_odd], quad_recv.at[8 + place_at])
        sides = []
        for parity in range(2):
            tiles = [last_in[parity, q // 2, q % 2].astype(F32) for q in range(4)]
            tiles = lanes_swapped(tiles)
            low = jnp.where(tp == 0, tiles[0], tiles[1])
            high = jnp.where(tp == 0, tiles[2], tiles[3])
            sides.append(jnp.where(odd == 0, low, high).reshape(8, 1, BLK, 128))
        both = jnp.concatenate(sides, axis=1).reshape(128, 128).T.astype(BF16)
        for q in range(4):
            out[:, 128 * q : 128 * q + 128] = both[32 * q : 32 * q + 32]

        arrived(mine, pair_sem.at[0])
        for n, (target, _) in enumerate(quad):
            arrived(tok.at[tp if n == 1 else other], quad_send.at[n])
            arrived(v_out.at[own_out], quad_send.at[3 + n])
            arrived(last_stage, quad_send.at[6 + n])
        everything = pl.ds(0, CHIPS - 1)
        for n, ref in (
            (0, buf_a), (1, part1), (2, buf_c), (3, incoming), (4, buf_m), (5, buf_g), (6, part2)
        ):
            arrived(ref.at[everything], send_sem.at[n])
        save.wait()


def run_layer(*arrays):
    bf, fl = BF16, F32
    dma = pltpu.SemaphoreType.DMA
    whole = (CHIPS, 2, 64, 128)
    in_vmem = pl.BlockSpec(memory_space=pltpu.VMEM)
    in_hbm = pl.BlockSpec(memory_space=pl.ANY)
    ff = 176
    eight = (8, 64, 128)
    sum_set = [
        pltpu.VMEM((2, *eight), bf), pltpu.VMEM((2, 2, *eight), bf), pltpu.VMEM((2, *eight), bf), pltpu.VMEM((2, *eight), bf),
        pltpu.VMEM((2, *eight), bf), pltpu.VMEM((2, *eight), bf), pltpu.VMEM((2, 4, 64, 128), bf),
    ]
    return pl.pallas_call(
        layer,
        out_shape=(
            jax.ShapeDtypeStruct((32, 512), bf),
            jax.ShapeDtypeStruct((HEADS, HEAD, HEAD), fl),
        ),
        in_specs=[pl.BlockSpec(memory_space=pltpu.HBM)] + [in_hbm] * 19,
        out_specs=(in_vmem, in_hbm),
        scratch_shapes=[
            pltpu.VMEM(whole, bf), pltpu.VMEM(whole, bf),
            pltpu.VMEM((CHIPS, 2, BLK, D // 2), bf), pltpu.VMEM(whole, bf),
            pltpu.VMEM((ROWS, 256), bf), pltpu.VMEM((ROWS, 128), fl),
            pltpu.VMEM((ROWS, ff), fl), pltpu.VMEM((ROWS, ff), fl), pltpu.VMEM((ROWS, 256 + 2 * HEADS), fl),
            pltpu.VMEM(whole, bf), pltpu.VMEM(whole, bf),
            *sum_set, *sum_set,
            *([pltpu.VMEM((ff, D), bf)] * 6),
            pltpu.VMEM((256 + 2 * HEADS, D), bf), pltpu.VMEM((128, D), bf),
            *([pltpu.VMEM((HEADS, HEAD, HEAD), fl)] * 2), *([pltpu.VMEM((128, 128), fl)] * 2), pltpu.VMEM((5, 128, 128), fl),
            pltpu.VMEM((32, 512), bf), pltpu.VMEM((1, HEADS), fl), pltpu.VMEM((3, 1, D), fl),
            pltpu.SMEM((1,), jnp.int32), pltpu.VMEM((CHIPS, 2, BLK, 128), bf), pltpu.VMEM((CHIPS, 2, BLK, 128), bf),
            pltpu.VMEM((ROWS, 2 * HEADS), fl), pltpu.VMEM((2, 64, 128), bf), pltpu.VMEM((4, 64, 128), bf),
            pltpu.VMEM((2, 64, 128), bf), pltpu.VMEM((2, 2, 2, 64, 128), bf),
            dma((21,)), dma((7,)), dma((4, 2, 32)), dma((2, 2, 40)), dma((32,)), dma((2,)), dma((9,)), dma((12,)),
        ],
        compiler_params=pltpu.CompilerParams(
            collective_id=0, has_side_effects=True, vmem_limit_bytes=60_000_000
        ),
        name="layer",
    )(*arrays)


def store(out, state, out_hbm, state_hbm, out_vmem, state_vmem, sems):
    pieces = [(out, out_vmem, out_hbm)]
    for n in range(4):
        heads = pl.ds(4 * n, 4)
        pieces.append((state.at[heads], state_vmem.at[heads], state_hbm.at[heads]))
    reads = [pltpu.make_async_copy(a, b, sems.at[0, n]) for n, (a, b, _) in enumerate(pieces)]
    writes = [pltpu.make_async_copy(b, c, sems.at[1, n]) for n, (_, b, c) in enumerate(pieces)]
    for read in reads:
        read.start()
    for read, write in zip(reads, writes):
        read.wait()
        write.start()
    for write in writes:
        write.wait()


def stored(out, state):
    anywhere = pl.BlockSpec(memory_space=pl.ANY)
    return pl.pallas_call(
        store,
        out_shape=(jax.ShapeDtypeStruct(out.shape, out.dtype), jax.ShapeDtypeStruct(state.shape, state.dtype)),
        in_specs=[anywhere] * 2,
        out_specs=(anywhere,) * 2,
        scratch_shapes=[
            pltpu.VMEM(out.shape, out.dtype), pltpu.VMEM(state.shape, state.dtype), pltpu.SemaphoreType.DMA((2, 5)),
        ],
        compiler_params=pltpu.CompilerParams(vmem_limit_bytes=60_000_000),
        name="store",
    )(out, state)


def per_device(
    tokens,
    lengths,
    state,
    gain_first,
    first_gate,
    first_up,
    first_down,
    gain_mix,
    query_weight,
    key_weight,
    value_weight,
    gating_weight,
    write_weight,
    forget_weight,
    forget_rate,
    out_weight,
    gain_second,
    second_gate,
    second_up,
    second_down,
):
    out, new_state = run_layer(
        lengths, tokens.T, forget_rate[None, :], gain_first[None, :], gain_mix[None, :], gain_second[None, :],
        first_gate.T, first_up.T, first_down, second_gate.T, second_up.T, second_down,
        query_weight.T, key_weight.T, value_weight.T, gating_weight.T, out_weight.T,
        write_weight.T, forget_weight.T, state.reshape(HEADS, HEAD, HEAD),
    )
    out, new_state = stored(out, new_state)
    return out.T, new_state.reshape(state.shape)


def solution(mesh):
    in_specs = (
        P("dp", ("kv", "tp")),
        P(("dp", "kv", "tp")),
        P(("dp", "kv", "tp"), None, None, None),
        P(),
        P(None, "kv"),
        P(None, "kv"),
        P("kv", None),
        P(),
        P(None, ("kv", "tp")),
        P(None, ("kv", "tp")),
        P(None, ("kv", "tp")),
        P(None, ("kv", "tp")),
        P(),
        P(),
        P(),
        P(None, ("kv", "tp")),
        P(),
        P(None, "kv"),
        P(None, "kv"),
        P("kv", None),
    )
    out_specs = (P("dp", ("kv", "tp")), P(("dp", "kv", "tp"), None, None, None))
    return jax.shard_map(
        per_device, mesh=mesh, in_specs=in_specs, out_specs=out_specs, check_vma=False
    )
```

```python
import math

import jax
import jax.numpy as jnp
from jax import lax
from jax.experimental import pallas as pl
from jax.experimental.pallas import tpu as pltpu
from jax.sharding import PartitionSpec as P

HEADS = 16
HEAD = 128
BLK = 8
D = 2048
NX = 4
NZ = 8
CHIPS = NX * NZ
ROWS = CHIPS * BLK
EPSILON = 1e-06
F32 = jnp.float32
BF16 = jnp.bfloat16
HIGH = lax.Precision.HIGHEST


def lanes_swapped(tiles):
    rows = tiles[0].shape[0]
    lane = lax.broadcasted_iota(jnp.int32, (rows, 128), 1)
    out = list(tiles)
    for step in (2, 1):
        width = step * 32
        low = (lane & width) == 0
        for i in range(4):
            if i & step:
                continue
            a, b = out[i], out[i + step]
            out[i] = jnp.where(low, a, pltpu.roll(b, width, 1))
            out[i + step] = jnp.where(low, pltpu.roll(a, 128 - width, 1), b)
    return out


def dot_nt(a, b, precision=None):
    return lax.dot_general(
        a, b, (((1,), (1,)), ((), ())), precision=precision, preferred_element_type=F32
    )


def wrapped(dz):
    return (dz + 3) % NZ - 3


def place(dx, dz):
    return (dx % NX) * NZ + dz % NZ


def children(half, dx, dz):
    sign = 1 if half == 0 else -1
    dx, dz = dx % NX, wrapped(dz)
    if abs(dz) == 1:
        return []
    found = []
    if dx == 0:
        found += [(sign, dz), (-sign, dz)]
        if dz == 0:
            found += [(0, 2), (0, -2), (0, 3), (0, -3), (0, 4), (0, 1), (0, -1)]
    else:
        if dx == sign % NX:
            found += [(2, dz)]
        if dz == 0:
            found += [(dx, 1), (dx, -1)]
    return found


GATHER_STEPS = (
    ("side", 0), ("column", 2), ("column", -2), ("far", 0), ("column", 3), ("column", -3), ("column", 4),
    ("relay", 2), ("row", 0), ("relay", -2), ("relay", 3), ("row", 1), ("relay", -3), ("relay", 4),
    ("row", -1), ("row", 2), ("row", -2), ("row", 3), ("row", -3), ("row", 4),
)
SUM_STEPS = (
    ("produce", 4), ("produce", 1), ("produce", -1), ("produce", 3), ("produce", -3),
    ("produce", 2), ("produce", -2), ("produce", 0),
    ("relay", 4), ("relay", 3), ("relay", -3), ("cross_row", 0), ("relay", 2), ("column", 4),
    ("relay", -2), ("column", 3), ("column", -3), ("relay", 0), ("column", 2), ("column", -2), ("column", 0),
)


class Torus:
    def __init__(self):
        self.kv = lax.axis_index("kv")
        self.tp = lax.axis_index("tp")
        self.x = lax.rem(self.kv, NX)
        self.z = lax.div(self.kv, NX)

    def at(self, dx, dz):
        return lax.rem(self.z + dz % NZ, NZ) * NX + lax.rem(self.x + dx % NX, NX)


def send(src, dst, send_sem, recv_sem, target):
    pltpu.make_async_remote_copy(
        src_ref=src,
        dst_ref=dst,
        send_sem=send_sem,
        recv_sem=recv_sem,
        device_id=target,
        device_id_type=pl.DeviceIdType.MESH,
    ).start()


def arrived(ref, sem):
    pltpu.make_async_copy(ref, ref, sem).wait()


def gather(torus, buf, send_sem, recv_sem, consume=None, started=None):
    def pass_on(half, dx, dz, only=None):
        source = torus.at(-dx, -dz)
        targets = children(half, dx, dz)
        for cx, cz in targets if only is None else targets[only : only + 1]:
            send(
                buf.at[source, half],
                buf.at[source, half],
                send_sem,
                recv_sem.at[half, place(cx, cz)],
                {"kv": torus.at(cx - dx, cz - dz)},
            )

    def take(half, dx, dz):
        arrived(buf.at[torus.at(-dx, -dz), half], recv_sem.at[half, place(dx, dz)])
        pass_on(half, dx, dz)

    for hop in range(len(children(0, 0, 0))):
        for half in range(2):
            pass_on(half, 0, 0, hop)
    if started is not None:
        started()
    for what, dz in GATHER_STEPS:
        if what == "column":
            take(0, 0, dz)
            take(1, 0, dz)
        elif what == "side":
            for dx in (1, -1):
                take(0, dx, 0)
                take(1, dx, 0)
        elif what == "far":
            take(0, 2, 0)
            take(1, 2, 0)
        elif what == "relay":
            take(0, 1, dz)
            take(1, -1, dz)
        else:
            if abs(dz) == 1:
                places = [(half, dx) for dx in (0, 1, -1, 2) for half in range(2)]
            elif dz != 0:
                places = [(0, -1), (1, 1), (0, 2), (1, 2)]
            else:
                places = []
            for half, dx in places:
                take(half, dx, dz)
            if consume is not None:
                consume(lax.rem(torus.z + (-dz) % NZ, NZ))


def sum_at_owner(
    torus, part, relay, column, final, along_z, stage_x, stage_z, stage_row, send_sem, recv_sem, produce
):
    sums = [None, None]

    def slot(dz):
        return dz % NZ

    def z_slot(dx, dz):
        return (dx % NX) + (0 if dz == 1 else NX)

    def term(half, dx, dz):
        total = part[torus.at(-dx, -dz), half].astype(F32)
        if dz == 0 and dx != 0:
            for side in (1, -1):
                total = total + along_z[half, z_slot(dx, side)].astype(F32)
        return total

    def post(src, dst, half, place_at, target):
        send(src, dst, send_sem, recv_sem.at[half, place_at], {"kv": target})

    def produce_step(dz):
        produce(lax.rem(torus.z + (-dz) % NZ, NZ))
        for half in range(2):
            if abs(dz) == 1:
                for dx in (2, 1, -1):
                    n = z_slot(dx, dz)
                    post(part.at[torus.at(-dx, -dz), half], along_z.at[half, n], half, 32 + n, torus.at(0, -dz))
                post(
                    part.at[torus.at(0, -dz), half], final.at[half, slot(dz)], half, 24 + slot(dz), torus.at(0, -dz)
                )
            elif dz != 0:
                for dx in (2, 1, -1):
                    to_column(half, dx, dz, part.at[torus.at(-dx, -dz), half])

    def to_column(half, dx, dz, src):
        sign = 1 if half == 0 else -1
        if dx == 2:
            post(src, relay.at[half, slot(dz)], half, slot(dz), torus.at(-sign, 0))
        elif dx == -sign:
            post(src, column.at[half, 0, slot(dz)], half, 8 + slot(dz), torus.at(sign, 0))

    def cross_row_step():
        for half in range(2):
            for dx in (2, 1, -1):
                for side in (1, -1):
                    n = z_slot(dx, side)
                    arrived(along_z.at[half, n], recv_sem.at[half, 32 + n])
        for half, dx in ((0, 2), (1, 2), (0, -1), (1, 1)):
            stage_row[half, dx % NX] = term(half, dx, 0).astype(BF16)
            to_column(half, dx, 0, stage_row.at[half, dx % NX])

    def relay_step(half, dz):
        sign = 1 if half == 0 else -1
        arrived(relay.at[half, slot(dz)], recv_sem.at[half, slot(dz)])
        total = term(half, sign, dz) + relay[half, slot(dz)].astype(F32)
        stage_x[half, slot(dz)] = total.astype(BF16)
        post(stage_x.at[half, slot(dz)], column.at[half, 1, slot(dz)], half, 16 + slot(dz), torus.at(-sign, 0))

    def column_step(half, dz):
        total = term(half, 0, dz)
        for n in range(2):
            arrived(column.at[half, n, slot(dz)], recv_sem.at[half, 8 + 8 * n + slot(dz)])
            total = total + column[half, n, slot(dz)].astype(F32)
        if dz == 0:
            sums[half] = total
            return
        stage_z[half, slot(dz)] = total.astype(BF16)
        post(stage_z.at[half, slot(dz)], final.at[half, slot(dz)], half, 24 + slot(dz), torus.at(0, -dz))

    for what, dz in SUM_STEPS:
        if what == "produce":
            produce_step(dz)
        elif what == "cross_row":
            cross_row_step()
        elif what == "relay":
            relay_step(0, dz)
            relay_step(1, dz)
        else:
            column_step(0, dz)
            column_step(1, dz)
    for dz in (1, -1, 4, 3, -3, 2, -2):
        for half in range(2):
            arrived(final.at[half, slot(dz)], recv_sem.at[half, 24 + slot(dz)])
            sums[half] = sums[half] + final[half, slot(dz)].astype(F32)
    return sums


def renew(h, state, fresh, update_refs):
    rows = slice(8 * h, 8 * h + 8)
    faded_ref, update_ref, kept_ref = update_refs
    gained = lax.dot_general(
        faded_ref[rows], update_ref[rows], (((0,), (0,)), ((), ())), precision=HIGH, preferred_element_type=F32
    )
    fresh[h] = kept_ref[8 * h : 8 * h + 1, :] * state[h] + gained


def unpack_row(buf, gain_ref, scaled_ref, squares_ref, zt):
    for tile in range(2):
        gain = gain_ref[:, pl.ds(pl.multiple_of(zt * 256 + 128 * tile, 128), 128)]
        for odd in range(2):
            for half in range(2):
                rows = slice(128 * odd + 64 * half, 128 * odd + 64 * half + 64)
                value = buf[4 * zt + 2 * tile + odd, half].astype(F32)
                scaled_ref[rows, 128 * tile : 128 * tile + 128] = (value * gain).astype(BF16)
                squares_ref[rows, :] += value * value


def scale_of(squares_ref):
    return lax.rsqrt(jnp.sum(squares_ref[...], axis=1, keepdims=True) / D + EPSILON)


def half_step(torus, buf, gain_ref, gate_ref, up_ref, down_ref, weight_waits, scaled_ref, squares_ref,
              acts, part, sum_refs, gather_sems, sum_sems, started=None, gathered=None):
    gate_act, up_act = acts
    squares_ref[...] = jnp.zeros_like(squares_ref)
    gate_act[...] = jnp.zeros_like(gate_act)
    up_act[...] = jnp.zeros_like(up_act)
    for wait in weight_waits:
        wait()

    def consume(zt):
        unpack_row(buf, gain_ref, scaled_ref, squares_ref, zt)
        channels = pl.ds(pl.multiple_of(zt * 256, 256), 256)
        scaled = scaled_ref[...]
        gate_act[...] += dot_nt(scaled, gate_ref[:, channels])
        up_act[...] += dot_nt(scaled, up_ref[:, channels])

    with jax.named_scope("gather"):
        gather(torus, buf, *gather_sems, consume, started)
    if gathered is not None:
        gathered()
    with jax.named_scope("units"):
        row_scale = scale_of(squares_ref)
        hidden = (jax.nn.silu(gate_act[...] * row_scale) * (up_act[...] * row_scale)).astype(BF16)

    def produce(zt):
        cols = pl.ds(pl.multiple_of(zt * 256, 256), 256)
        product = jnp.dot(hidden, down_ref[:, cols], preferred_element_type=F32)
        for tile in range(2):
            for odd in range(2):
                for half in range(2):
                    row = 128 * odd + 64 * half
                    block = product[row : row + 64, 128 * tile : 128 * tile + 128]
                    part[4 * zt + 2 * tile + odd, half] = block.astype(BF16)

    with jax.named_scope("sum"):
        return sum_at_owner(torus, part, *sum_refs, *sum_sems, produce)


def spread(rows):
    parts = [jnp.broadcast_to(rows[:, h : h + 1], (BLK, 128)) for h in range(HEADS)]
    return jnp.concatenate(parts, axis=0)


def decays(write_pre, forget_pre, rates, live):
    live_heads = live[:, :HEADS]
    write = spread(jax.nn.sigmoid(write_pre) * live_heads)
    forget = spread(-jnp.exp(rates) * jax.nn.softplus(forget_pre) * live_heads)
    row = lax.broadcasted_iota(jnp.int32, (128, 128), 0)
    col = lax.broadcasted_iota(jnp.int32, (128, 128), 1)
    causal = ((row >> 3) == (col >> 3)) & (col <= row)
    cumulative = jnp.dot(
        jnp.where(causal, 1.0, 0.0), forget, precision=HIGH, preferred_element_type=F32
    )
    decay = jnp.where(causal, jnp.exp(jnp.minimum(cumulative - cumulative.T, 0.0)), 0.0)
    by_head = cumulative.reshape(HEADS, BLK, 128)
    last = by_head[:, BLK - 1 : BLK, :]
    fading = jnp.exp(last - by_head).reshape(128, 128)
    kept = jnp.broadcast_to(jnp.exp(last), (HEADS, BLK, 128)).reshape(128, 128)
    return write, jnp.exp(cumulative), decay, fading, kept


def delta(owned, decays_ref, live, state, update_refs):
    query, key, value, gating = owned
    write, growth, decay = decays_ref[0], decays_ref[1], decays_ref[2]
    query_unit = query * lax.rsqrt(jnp.sum(query * query, axis=1, keepdims=True) + EPSILON)
    query_unit = query_unit / math.sqrt(HEAD)
    key_unit = key * lax.rsqrt(jnp.sum(key * key, axis=1, keepdims=True) + EPSILON)
    row = lax.broadcasted_iota(jnp.int32, (128, 128), 0)
    col = lax.broadcasted_iota(jnp.int32, (128, 128), 1)
    strict = col < row
    identity = jnp.where(row == col, 1.0, 0.0)

    def dot(a, b):
        return jnp.dot(a, b, precision=HIGH, preferred_element_type=F32)

    products = dot_nt(jnp.concatenate([key_unit, query_unit], axis=0), key_unit, HIGH)
    strict_part = jnp.where(strict, write * decay * products[:128], 0.0)
    squared = dot(strict_part, strict_part)
    fourth = dot(squared, squared)
    inverse = dot(dot(identity - strict_part, identity + squared), identity + fourth)
    solved = dot(inverse, jnp.concatenate([write * value, write * growth * key_unit], axis=1))
    target, key_mix = solved[:, :128], solved[:, 128:]
    scores = products[128:] * decay
    grown = query_unit * growth
    faded = key_unit * decays_ref[3]
    updates, reads = [], []
    for h in range(HEADS):
        rows = slice(8 * h, 8 * h + 8)
        both = jnp.concatenate([key_mix[rows], grown[rows]], axis=0)
        seen = dot(both, state[h])
        updates.append(target[rows] - seen[:BLK])
        reads.append(seen[BLK:])
    update = jnp.concatenate(updates, axis=0)
    faded_ref, update_ref, _ = update_refs
    faded_ref[...] = faded
    update_ref[...] = update
    attend = jnp.concatenate(reads, axis=0) + dot(scores, update)
    normed = attend * lax.rsqrt(jnp.mean(attend * attend, axis=1, keepdims=True) + EPSILON)
    return normed * jax.nn.silu(gating) * jnp.concatenate([live] * HEADS, axis=0)


def layer(
    length, tokens, rates, gain_first, gain_mix, gain_second,
    gate1, up1, down1, gate2, up2, down2, query, key, value, gating, outw, writew, forgetw, state,
    out, new_state,
    buf_a, buf_c, buf_m, buf_g, scaled, squares, gate_act, up_act, project, part1, part2,
    relay1, column1, final1, along1, stage_x1, stage_z1, stage_row1,
    relay2, column2, final2, along2, stage_x2, stage_z2, stage_row2,
    v_gate1, v_up1, v_down1, v_gate2, v_up2, v_down2, v_all, v_out, v_state, v_fresh, faded_s, update_s, decays_s,
    v_tokens, v_rates, v_gains, s_length, outgoing, incoming, gates, tok, tok_in, last_stage, last_in,
    local_sem, send_sem, recv_ag, recv_rs, recv_x, pair_sem, quad_send, quad_recv,
):
    torus = Torus()
    update_refs = (faded_s, update_s, decays_s.at[4])

    def own_columns(t):
        return pl.multiple_of(128 * t, 128)

    kv, tp = torus.kv, torus.tp
    other = 1 - tp
    odd = lax.rem(kv, 2)
    twin = kv + 1 - 2 * odd
    seat = 2 * odd + tp
    own_out = pl.ds(pl.multiple_of(32 * seat, 32), 32)
    quad = [
        ({"tp": other}, 2 * odd + other),
        ({"kv": twin}, 2 * (1 - odd) + tp),
        ({"kv": twin, "tp": other}, 2 * (1 - odd) + other),
    ]

    with jax.named_scope("entry"):
        barrier = pltpu.get_barrier_semaphore()
        near = [{"kv": torus.at(dx, 0)} for dx in (1, -1)]
        near += [{"kv": torus.at(0, dz)} for dz in (1, -1, 2, -2, 3, -3, 4)]
        near += [{"tp": other}, {"kv": twin, "tp": other}]
        for target in near:
            pl.semaphore_signal(barrier, inc=1, device_id=target, device_id_type=pl.DeviceIdType.MESH)
        loads = {}
        for n, (name, src, dst) in enumerate(
            [
                ("tokens", tokens, v_tokens), ("gain1", gain_first, v_gains.at[0]),
                ("gate1", gate1, v_gate1), ("up1", up1, v_up1), ("down1", down1, v_down1),
                ("query", query, v_all.at[pl.ds(own_columns(tp), 32)]),
                ("key", key, v_all.at[pl.ds(own_columns(tp) + 32, 32)]),
                ("value", value, v_all.at[pl.ds(own_columns(tp) + 64, 32)]),
                ("gating", gating, v_all.at[pl.ds(own_columns(tp) + 96, 32)]),
                ("out", outw, v_out.at[own_out]),
                ("write", writew, v_all.at[256:272]), ("forget", forgetw, v_all.at[272:288]),
                ("state", state, v_state),
                ("length", length, s_length), ("rates", rates, v_rates),
                ("gain_mix", gain_mix, v_gains.at[1]), ("gain2", gain_second, v_gains.at[2]),
                ("gate2", gate2, v_gate2), ("up2", up2, v_up2), ("down2", down2, v_down2),
            ]
        ):
            loads[name] = pltpu.make_async_copy(src, dst, local_sem.at[n])
            loads[name].start()

        loads["tokens"].wait()
        values = v_tokens[...].astype(F32)
        values = jnp.concatenate([values[:, 128 * q : 128 * q + 128] for q in range(4)], axis=0).T
        values = values.reshape(8, 2, BLK, 128)
        for parity in range(2):
            tok[parity] = values[:, parity].reshape(64, 128).astype(BF16)
        pl.semaphore_wait(barrier, len(near))
    with jax.named_scope("quad_in"):
        for n, (target, _) in enumerate(quad):
            row = tp if n == 1 else other
            send(tok.at[row], tok_in.at[seat], quad_send.at[n], quad_recv.at[seat], target)
        tok_in[seat] = tok[tp]
        for _, place_at in quad:
            arrived(tok_in.at[place_at], quad_recv.at[place_at])
        tiles = lanes_swapped([tok_in[j].astype(F32) for j in range(4)])
        for half in range(2):
            buf_a[kv, half] = jnp.where(odd == 0, tiles[half], tiles[2 + half]).astype(BF16)
    mine = v_all.at[pl.ds(own_columns(tp), 128)]

    def share_out():
        loads["out"].wait()
        send(v_out.at[own_out], v_out.at[own_out], quad_send.at[4], quad_recv.at[4 + seat], {"kv": twin})

    def share_projections():
        for name in ("query", "key", "value", "gating"):
            loads[name].wait()
        send(v_out.at[own_out], v_out.at[own_out], quad_send.at[3], quad_recv.at[4 + seat], {"tp": other})
        send(mine, mine, pair_sem.at[0], pair_sem.at[1], {"tp": other})

    sums = half_step(
        torus, buf_a, v_gains.at[0], v_gate1, v_up1, v_down1,
        [loads["gain1"].wait, loads["gate1"].wait, loads["up1"].wait, loads["down1"].wait],
        scaled, squares, (gate_act, up_act), part1,
        (relay1, column1, final1, along1, stage_x1, stage_z1, stage_row1),
        (send_sem.at[0], recv_ag.at[0]), (send_sem.at[1], recv_rs.at[0]), share_out, share_projections,
    )
    for half in range(2):
        buf_c[kv, half] = (buf_a[kv, half].astype(F32) + 0.5 * sums[half]).astype(BF16)

    arrived(v_all.at[pl.ds(own_columns(other), 128)], pair_sem.at[1])
    loads["write"].wait()
    loads["gain_mix"].wait()
    loads["forget"].wait()
    squares[...] = jnp.zeros_like(squares)
    project[...] = jnp.zeros_like(project)

    def consume(zt):
        unpack_row(buf_c, v_gains.at[1], scaled, squares, zt)
        channels = pl.ds(pl.multiple_of(zt * 256, 256), 256)
        project[...] += dot_nt(scaled[...], v_all[:, channels])

    with jax.named_scope("gather_c"):
        gather(torus, buf_c, send_sem.at[2], recv_ag.at[1], consume)
    with jax.named_scope("project"):
        mix_scale = scale_of(squares)
        for t in range(2):
            product = project[:, 128 * t : 128 * t + 128] * mix_scale
            outgoing[:, t] = product.reshape(CHIPS, BLK, 128).astype(BF16)
        gates[...] = project[:, 256:] * mix_scale
    with jax.named_scope("exchange"):
        offsets = [(dx, dz) for dz in (4, 3, -3, 2, -2, 1, -1, 0) for dx in (2, 1, -1, 0)][:-1]
        for dx, dz in offsets:
            peer = torus.at(dx, dz)
            send(outgoing.at[peer], incoming.at[kv], send_sem.at[3], recv_x.at[place(dx, dz)], {"kv": peer})
        incoming[kv] = outgoing[kv]
        own_rows = pl.ds(pl.multiple_of(kv * BLK, BLK), BLK)
        loads["length"].wait()
        position = lax.broadcasted_iota(jnp.int32, (BLK, 128), 0)
        live = jnp.where(position < s_length[0], 1.0, 0.0)
        loads["state"].wait()
        loads["rates"].wait()
        gates_in = gates[own_rows, :]
        for n, value in enumerate(decays(gates_in[:, :HEADS], gates_in[:, HEADS:], v_rates[...], live)):
            decays_s[n] = value
        for dx, dz in offsets:
            arrived(incoming.at[torus.at(-dx, -dz)], recv_x.at[place(dx, dz)])
    twin_seat = quad[1][1]
    twin_out = v_out.at[pl.ds(pl.multiple_of(32 * twin_seat, 32), 32)]
    with jax.named_scope("delta"):
        tiles = incoming[...].astype(F32).reshape(HEADS, 4, BLK, 128)
        owned = lanes_swapped([tiles[:, j].reshape(128, 128) for j in range(4)])
        mixed = delta(owned, decays_s, live, v_state, update_refs)
        for h in range(HEADS):
            lanes = slice(128 * (h % 8), 128 * (h % 8) + 128)
            buf_m[kv, h // 8, :, lanes] = mixed[8 * h : 8 * h + 8].astype(BF16)
    heads_left = list(range(HEADS))

    def renew_two(zt):
        if len(heads_left) == HEADS:
            arrived(twin_out, quad_recv.at[4 + twin_seat])
            send(twin_out, twin_out, quad_send.at[5], quad_recv.at[4 + twin_seat], {"tp": other})
        for _ in range(2):
            renew(heads_left.pop(0), v_state, v_fresh, update_refs)

    with jax.named_scope("gather_m"):
        gather(torus, buf_m, send_sem.at[4], recv_ag.at[2], renew_two)
    save = pltpu.make_async_copy(v_fresh, new_state, local_sem.at[20])
    save.start()
    with jax.named_scope("out_product"):
        for place_at in (quad[0][1], quad[2][1]):
            rows = pl.ds(pl.multiple_of(32 * place_at, 32), 32)
            arrived(v_out.at[rows], quad_recv.at[4 + place_at])
        mixed_sum = jnp.zeros((128, 128), F32)
        for half in range(2):
            lanes = slice(half * (D // 2), (half + 1) * (D // 2))
            heads_half = buf_m[pl.ds(16 * odd, 16), half].astype(F32).reshape(128, D // 2).astype(BF16)
            mixed_sum = mixed_sum + dot_nt(heads_half, v_out[:, lanes]).astype(BF16).astype(F32)
        for half in range(2):
            rows = slice(64 * half, 64 * half + 64)
            buf_g[kv, half] = (buf_c[kv, half].astype(F32) + mixed_sum[rows]).astype(BF16)

    sums = half_step(
        torus, buf_g, v_gains.at[2], v_gate2, v_up2, v_down2,
        [loads["gain2"].wait, loads["gate2"].wait, loads["up2"].wait, loads["down2"].wait],
        scaled, squares, (gate_act, up_act), part2,
        (relay2, column2, final2, along2, stage_x2, stage_z2, stage_row2),
        (send_sem.at[5], recv_ag.at[3]), (send_sem.at[6], recv_rs.at[1]),
    )
    with jax.named_scope("finish"):
        for half in range(2):
            last_stage[half] = (buf_g[kv, half].astype(F32) + 0.5 * sums[half]).astype(BF16)
        for n, (target, _) in enumerate(quad):
            send(last_stage, last_in.at[tp, odd], quad_send.at[6 + n], quad_recv.at[8 + 2 * odd + tp], target)
        last_in[tp, odd] = last_stage[...]
        for _, place_at in quad:
            from_odd, from_tp = lax.div(place_at, 2), lax.rem(place_at, 2)
            arrived(last_in.at[from_tp, from_odd], quad_recv.at[8 + place_at])
        sides = []
        for parity in range(2):
            tiles = [last_in[parity, q // 2, q % 2].astype(F32) for q in range(4)]
            tiles = lanes_swapped(tiles)
            low = jnp.where(tp == 0, tiles[0], tiles[1])
            high = jnp.where(tp == 0, tiles[2], tiles[3])
            sides.append(jnp.where(odd == 0, low, high).reshape(8, 1, BLK, 128))
        both = jnp.concatenate(sides, axis=1).reshape(128, 128).T.astype(BF16)
        for q in range(4):
            out[:, 128 * q : 128 * q + 128] = both[32 * q : 32 * q + 32]

        arrived(mine, pair_sem.at[0])
        for n, (target, _) in enumerate(quad):
            arrived(tok.at[tp if n == 1 else other], quad_send.at[n])
            arrived(v_out.at[own_out], quad_send.at[3 + n])
            arrived(last_stage, quad_send.at[6 + n])
        everything = pl.ds(0, CHIPS - 1)
        for n, ref in (
            (0, buf_a), (1, part1), (2, buf_c), (3, incoming), (4, buf_m), (5, buf_g), (6, part2)
        ):
            arrived(ref.at[everything], send_sem.at[n])
        save.wait()


def run_layer(*arrays):
    bf, fl = BF16, F32
    dma = pltpu.SemaphoreType.DMA
    whole = (CHIPS, 2, 64, 128)
    in_vmem = pl.BlockSpec(memory_space=pltpu.VMEM)
    in_hbm = pl.BlockSpec(memory_space=pl.ANY)
    ff = 176
    eight = (8, 64, 128)
    sum_set = [
        pltpu.VMEM((2, *eight), bf), pltpu.VMEM((2, 2, *eight), bf), pltpu.VMEM((2, *eight), bf), pltpu.VMEM((2, *eight), bf),
        pltpu.VMEM((2, *eight), bf), pltpu.VMEM((2, *eight), bf), pltpu.VMEM((2, 4, 64, 128), bf),
    ]
    return pl.pallas_call(
        layer,
        out_shape=(
            jax.ShapeDtypeStruct((32, 512), bf),
            jax.ShapeDtypeStruct((HEADS, HEAD, HEAD), fl),
        ),
        in_specs=[pl.BlockSpec(memory_space=pltpu.HBM)] + [in_hbm] * 19,
        out_specs=(in_vmem, in_hbm),
        scratch_shapes=[
            pltpu.VMEM(whole, bf), pltpu.VMEM(whole, bf),
            pltpu.VMEM((CHIPS, 2, BLK, D // 2), bf), pltpu.VMEM(whole, bf),
            pltpu.VMEM((ROWS, 256), bf), pltpu.VMEM((ROWS, 128), fl),
            pltpu.VMEM((ROWS, ff), fl), pltpu.VMEM((ROWS, ff), fl), pltpu.VMEM((ROWS, 256 + 2 * HEADS), fl),
            pltpu.VMEM(whole, bf), pltpu.VMEM(whole, bf),
            *sum_set, *sum_set,
            *([pltpu.VMEM((ff, D), bf)] * 6),
            pltpu.VMEM((256 + 2 * HEADS, D), bf), pltpu.VMEM((128, D), bf),
            *([pltpu.VMEM((HEADS, HEAD, HEAD), fl)] * 2), *([pltpu.VMEM((128, 128), fl)] * 2), pltpu.VMEM((5, 128, 128), fl),
            pltpu.VMEM((32, 512), bf), pltpu.VMEM((1, HEADS), fl), pltpu.VMEM((3, 1, D), fl),
            pltpu.SMEM((1,), jnp.int32), pltpu.VMEM((CHIPS, 2, BLK, 128), bf), pltpu.VMEM((CHIPS, 2, BLK, 128), bf),
            pltpu.VMEM((ROWS, 2 * HEADS), fl), pltpu.VMEM((2, 64, 128), bf), pltpu.VMEM((4, 64, 128), bf),
            pltpu.VMEM((2, 64, 128), bf), pltpu.VMEM((2, 2, 2, 64, 128), bf),
            dma((21,)), dma((7,)), dma((4, 2, 32)), dma((2, 2, 40)), dma((32,)), dma((2,)), dma((9,)), dma((12,)),
        ],
        compiler_params=pltpu.CompilerParams(
            collective_id=0, has_side_effects=True, vmem_limit_bytes=60_000_000
        ),
        name="layer",
    )(*arrays)


def store(out, state, out_hbm, state_hbm, out_vmem, state_vmem, sems):
    pieces = [(out, out_vmem, out_hbm)]
    for n in range(4):
        heads = pl.ds(4 * n, 4)
        pieces.append((state.at[heads], state_vmem.at[heads], state_hbm.at[heads]))
    reads = [pltpu.make_async_copy(a, b, sems.at[0, n]) for n, (a, b, _) in enumerate(pieces)]
    writes = [pltpu.make_async_copy(b, c, sems.at[1, n]) for n, (_, b, c) in enumerate(pieces)]
    for read in reads:
        read.start()
    for read, write in zip(reads, writes):
        read.wait()
        write.start()
    for write in writes:
        write.wait()


def stored(out, state):
    anywhere = pl.BlockSpec(memory_space=pl.ANY)
    return pl.pallas_call(
        store,
        out_shape=(jax.ShapeDtypeStruct(out.shape, out.dtype), jax.ShapeDtypeStruct(state.shape, state.dtype)),
        in_specs=[anywhere] * 2,
        out_specs=(anywhere,) * 2,
        scratch_shapes=[
            pltpu.VMEM(out.shape, out.dtype), pltpu.VMEM(state.shape, state.dtype), pltpu.SemaphoreType.DMA((2, 5)),
        ],
        compiler_params=pltpu.CompilerParams(vmem_limit_bytes=60_000_000),
        name="store",
    )(out, state)


def per_device(
    tokens,
    lengths,
    state,
    gain_first,
    first_gate,
    first_up,
    first_down,
    gain_mix,
    query_weight,
    key_weight,
    value_weight,
    gating_weight,
    write_weight,
    forget_weight,
    forget_rate,
    out_weight,
    gain_second,
    second_gate,
    second_up,
    second_down,
):
    out, new_state = run_layer(
        lengths, tokens.T, forget_rate[None, :], gain_first[None, :], gain_mix[None, :], gain_second[None, :],
        first_gate.T, first_up.T, first_down, second_gate.T, second_up.T, second_down,
        query_weight.T, key_weight.T, value_weight.T, gating_weight.T, out_weight.T,
        write_weight.T, forget_weight.T, state.reshape(HEADS, HEAD, HEAD),
    )
    out, new_state = stored(out, new_state)
    return out.T, new_state.reshape(state.shape)


def solution(mesh):
    in_specs = (
        P("dp", ("kv", "tp")),
        P(("dp", "kv", "tp")),
        P(("dp", "kv", "tp"), None, None, None),
        P(),
        P(None, "kv"),
        P(None, "kv"),
        P("kv", None),
        P(),
        P(None, ("kv", "tp")),
        P(None, ("kv", "tp")),
        P(None, ("kv", "tp")),
        P(None, ("kv", "tp")),
        P(),
        P(),
        P(),
        P(None, ("kv", "tp")),
        P(),
        P(None, "kv"),
        P(None, "kv"),
        P("kv", None),
    )
    out_specs = (P("dp", ("kv", "tp")), P(("dp", "kv", "tp"), None, None, None))
    return jax.shard_map(
        per_device, mesh=mesh, in_specs=in_specs, out_specs=out_specs, check_vma=False
    )
```
